256 devices in a mesh: fs: 32 (over z, y), tp: 8 (over x, core).
Axes of the slice: x: 4, y: 4, z: 8, core: 2. Of those that a mesh axis runs over, the one named last changes fastest.
Arguments:
- tokens: bfloat16 [12288, 2048], P('fs', 'tp'), may hold values from -6 to 6
- norm_gain: float32 [2048], P('fs'), may hold values from 0.1 to 1.9
- gate_train: bfloat16 [8, 2048, 5632], P(None, 'fs', 'tp'), may hold values from -0.125 to 0.125
- up_train: bfloat16 [8, 2048, 5632], P(None, 'fs', 'tp'), may hold values from -0.125 to 0.125
- down_train: bfloat16 [8, 2048, 5632], P(None, 'fs', 'tp'), may hold values from -0.078125 to 0.078125
- routes: int32 [12288, 2], P('fs'), may hold values from 0 to 7, all different within a row; in each aligned block of 384 rows (0 to 383, 384 to 767, ...) at most 192 rows name the same one
- route_logits: float32 [12288, 2], P('fs'), may hold values from -6 to 6
Outputs:
- gate_weights: bfloat16 [32, 2048, 5632], P('fs', None, 'tp')
- up_weights: bfloat16 [32, 2048, 5632], P('fs', None, 'tp')
- down_weights: bfloat16 [32, 2048, 5632], P('fs', None, 'tp')
- mixed: bfloat16 [12288, 2048], P('fs', 'tp')
The draws below stay inside these ranges and needn't reach their ends.
Inputs may be any that keep to these rules, and one draw needn't show every extreme that they name: `routes`: each row names 2 different experts; among the rows of one device no expert is named more than 192 times, and in every draw some device names some expert exactly 192 times.
All inputs are finite; a program needn't handle non-finite values.
Results may differ from the reference program's by a relative error of at most 0.014.
Values may be sent and summed in bfloat16 or wider, within the bound.
A program may use at most 128 MiB of HBM per device.

```python
import math
import jax
import jax.numpy as jnp
import numpy as np
from jax import lax

D = 2048
FF = 5632
EXPERTS = 8
TOP = 2
TOK_DEV = 384
TOKENS = 12288
MOST = 192
N_FS = 32
N_TP = 8


def levels(stream_key, shape, cuts, least, high):
    loudness = 1.0
    for axis_at, parts in cuts:
        heights = jax.random.uniform(jax.random.fold_in(jax.random.fold_in(stream_key, 6), axis_at), (parts,), jnp.float32, least / len(cuts), high / len(cuts))
        loudness = loudness * jnp.repeat(jnp.exp(heights), shape[axis_at] // parts).reshape((-1,) + (1,) * (len(shape) - 1 - axis_at))
    return loudness


def shared_out(stream_key, own, number, rows, amount, top, reach, lean):
    ranking = jax.random.permutation(stream_key, amount)
    crowded, ordinary = load_shares(amount, rows * top, reach, lean, True), load_shares(amount, rows * top, reach, lean, False)
    places = jnp.arange(amount)

    def named(tallies, offset_by):
        used = int((tallies > 0).sum())
        fixed = max(1, used // 4)
        moved = fixed + (places - fixed + offset_by * (used - fixed)) % max(1, amount - fixed)
        return jnp.zeros((amount,), jnp.int32).at[ranking[jnp.where(places < fixed, places, moved)]].set(jnp.asarray(tallies, jnp.int32))

    tallies = jnp.where(number % 4 == 0, named(crowded, number // 4), named(ordinary, number - number // 4 - 1))
    mixed = jax.random.permutation(jax.random.fold_in(own, 3), amount)
    giver, taker = mixed[0:amount // 2 * 2:2], mixed[1:amount // 2 * 2:2]
    slack = jnp.minimum(tallies[giver] - 1, reach - tallies[taker]) // 2
    slack = jnp.where((giver == ranking[0]) | (taker == ranking[0]) | (tallies[taker] == 0), 0, jnp.maximum(slack, 0))
    moved = jax.random.randint(jax.random.fold_in(own, 4), (amount // 2,), 0, 1 << 20) % (slack + 1)
    tallies = tallies.at[giver].add(-moved).at[taker].add(moved)
    labels = jnp.searchsorted(jnp.cumsum(tallies), jnp.arange(rows * top), side="right").astype(jnp.int32)
    table = labels.reshape(top, rows).T
    table = table[jax.random.permutation(jax.random.fold_in(own, 1), rows)]
    offset_by = jax.random.randint(jax.random.fold_in(own, 2), (rows, 1), 0, top)
    return jnp.take_along_axis(table, (jnp.arange(top)[None, :] + offset_by) % top, axis=1)


def load_shares(count, total, bound, slope, full):
    weights = [(1 << 20) // math.isqrt(grade ** slope) + 1 for grade in range(1, count + 1)]
    largest = bound if full else min(bound, max(-(-total // count), total * weights[0] // sum(weights)))
    least = 1 if total - largest >= count - 1 else 0
    given, spare = [largest] + [least] * (count - 1), total - largest - least * (count - 1)
    while spare > 0:
        free = [i for i in range(1, count) if given[i] < largest] or [i for i in range(1, count) if given[i] < bound]
        pool, budget = sum([weights[i] for i in free]), spare
        for i in free:
            more = min(bound - given[i], max(1, budget * weights[i] // pool), spare)
            given[i] = given[i] + more
            spare = spare - more
    return np.array(given)


def scatter_about(key, shape, deviation, limit, cuts=(), held_as=jnp.bfloat16):
    values = deviation * jax.random.normal(key, shape, jnp.float32)
    if cuts:
        values = values * levels(key, shape, cuts, -0.22, 0.18)
    return jnp.clip(values, -limit, limit).astype(held_as)


def setup_inputs(seed: int = 0) -> dict:
    key_list = jax.random.split(jax.random.key(seed), 8)
    tokens = scatter_about(key_list[0], (TOKENS, D), 1.0, 6.0, ((0, 32), (1, 8)))
    norm_gain = jnp.clip(1.0 + 0.18 * jax.random.normal(key_list[1], (D,), jnp.float32), 0.1, 1.9)
    gate_train = scatter_about(key_list[2], (EXPERTS, D, FF), D ** -0.5, 0.125, ((1, 32), (2, 8)))
    up_train = scatter_about(key_list[3], (EXPERTS, D, FF), D ** -0.5, 0.125, ((1, 32), (2, 8)))
    down_train = scatter_about(key_list[4], (EXPERTS, D, FF), FF ** -0.5, 0.078125, ((1, 32), (2, 8)))
    routes_keys = jax.random.split(jax.random.fold_in(key_list[5], 1), TOKENS // TOK_DEV)
    routes_turns = jax.random.permutation(jax.random.fold_in(key_list[5], 3), TOKENS // TOK_DEV)
    routes = jax.vmap(lambda own, number: shared_out(jax.random.fold_in(key_list[5], 2), own, number, TOK_DEV, EXPERTS, TOP, TOK_DEV // 2, 1))(routes_keys, routes_turns).reshape((TOKENS, TOP))
    route_logits = scatter_about(key_list[6], (TOKENS, TOP), 1.5, 6.0, ((0, 32),), jnp.float32)
    return {"tokens": tokens, "norm_gain": norm_gain, "gate_train": gate_train, "up_train": up_train, "down_train": down_train, "routes": routes, "route_logits": route_logits}


def reference(tokens, norm_gain, gate_train, up_train, down_train, routes, route_logits):
    slot_expert = jnp.arange(N_FS, dtype=jnp.int32) % EXPERTS
    gain_rows = norm_gain[None, :, None]
    gate_low = (gate_train.astype(jnp.float32) * gain_rows).astype(jnp.bfloat16)
    up_low = (up_train.astype(jnp.float32) * gain_rows).astype(jnp.bfloat16)
    down_low = down_train.astype(jnp.bfloat16)
    gate_weights = gate_low[slot_expert]
    up_weights = up_low[slot_expert]
    down_weights = down_low[slot_expert]
    tok_float = tokens.astype(jnp.float32)
    inverse = lax.rsqrt(lax.optimization_barrier(jnp.mean(tok_float * tok_float, axis=1, keepdims=True)) + 1e-06)
    normed = (tok_float * inverse).astype(jnp.bfloat16)
    padded = jnp.concatenate([normed, jnp.zeros((1, D), jnp.bfloat16)], axis=0)
    by_device = routes.reshape(N_FS, TOK_DEV * TOP)
    onehot = (by_device[:, :, None] == jnp.arange(EXPERTS, dtype=jnp.int32)[None, None, :]).astype(jnp.int32)
    order_rank = lax.optimization_barrier(jnp.sum((jnp.cumsum(onehot, axis=1) - onehot) * onehot, axis=2))
    position = (jnp.arange(N_FS, dtype=jnp.int32)[:, None] * MOST + order_rank).reshape(-1).astype(jnp.int32)
    flat_routes = by_device.reshape(-1)
    token_of = (jnp.arange(TOKENS * TOP, dtype=jnp.int32) // TOP).astype(jnp.int32)
    width = FF // N_TP
    results = []
    for expert in range(EXPERTS):
        spots = jnp.where(flat_routes == expert, position, N_FS * MOST).astype(jnp.int32)
        table = jnp.full((N_FS * MOST,), TOKENS, jnp.int32).at[spots].set(token_of, mode='drop')
        rows_in = padded[table]
        gate_val = jnp.dot(rows_in, gate_low[expert], preferred_element_type=jnp.float32)
        up_val = jnp.dot(rows_in, up_low[expert], preferred_element_type=jnp.float32)
        active = (jax.nn.silu(gate_val) * up_val).astype(jnp.bfloat16)
        total = jnp.zeros((N_FS * MOST, D), jnp.float32)
        for block in range(N_TP):
            partial_value = lax.dot_general(active[:, block * width:(block + 1) * width], down_low[expert][:, block * width:(block + 1) * width], (((1,), (1,)), ((), ())), preferred_element_type=jnp.float32)
            rounded = lax.optimization_barrier(partial_value.astype(jnp.bfloat16))
            total = total + rounded.astype(jnp.float32)
        results.append(total.astype(jnp.bfloat16))
    stacked = jnp.stack(results, axis=0)
    picked = stacked[flat_routes, position].astype(jnp.float32).reshape(TOKENS, TOP, D)
    first = jax.nn.sigmoid(route_logits[:, 0] - route_logits[:, 1])
    second = jax.nn.sigmoid(route_logits[:, 1] - route_logits[:, 0])
    mixed = (picked[:, 0, :] * first[:, None] + picked[:, 1, :] * second[:, None]).astype(jnp.bfloat16)
    return (gate_weights, up_weights, down_weights, mixed)
```

```python
import functools

import jax
import jax.numpy as jnp
from jax import lax
from jax.experimental import pallas as pl
from jax.experimental.pallas import tpu as pltpu
from jax.sharding import PartitionSpec as P

EXPERTS = 8
epsilon = 1e-06
MESH = pl.DeviceIdType.MESH
NZ, NY = 8, 4
PARTS = ((0, 384), (384, 320))


def weights_kernel(g_ref, u_ref, d_ref, og, ou, od, y0, y1, away, ysend, yrecv, zsend, zrecv):
    fs = lax.axis_index("fs")
    z, y = fs // NY, lax.rem(fs, NY)
    parity = lax.rem(z, 2)
    sources, outs, ybufs = (g_ref, u_ref, d_ref), (og, ou, od), (y0, y1)
    rows = g_ref.shape[2]

    def zat(step):
        return lax.rem(z + step + NZ, NZ)

    def yat(step):
        return lax.rem(y + step + NY, NY)

    def device(dz, dy):
        return {"fs": zat(dz) * NY + yat(dy)}

    barrier = pltpu.get_barrier_semaphore()
    partners = [(0, 1), (0, 2), (0, 3), (1, 0), (-1, 0), (2, 0), (-2, 0)]
    for dz, dy in partners:
        pl.semaphore_signal(barrier, inc=1, device_id=device(dz, dy), device_id_type=MESH)
    pl.semaphore_wait(barrier, len(partners))

    units = [(m, h) for m in range(3) for h in range(2)]

    def ycopy(u, dy, to_row):
        m, h = units[u]
        lo, n = PARTS[h]
        return pltpu.make_async_remote_copy(
            src_ref=sources[m].at[:, yat(dy), :, pl.ds(lo, n)],
            dst_ref=ybufs[h].at[m, :, pl.ds(to_row * rows, rows), :],
            send_sem=ysend.at[u * 3 + dy - 1],
            recv_sem=yrecv.at[u * 3 + dy - 1],
            device_id=device(0, dy),
            device_id_type=MESH,
        )

    def zcopy(u, kind, sign, arriving=False):
        m, h = units[u]
        lo, n = PARTS[h]
        out = outs[m]
        near = {"a": 1, "b": 2, "c": 2, "d": 2}[kind]
        hops = {"a": 0, "b": 0, "c": 1, "d": 2}[kind]
        block = zat(-sign * hops)
        if arriving:
            block = zat(-sign * (hops + near))
        if kind == "d":
            half = n // 2
            lo, n = (lo, half) if sign > 0 else (lo + half, half)
        place = out.at[block, pl.ds(lo, n), :]
        source = away.at[m, pl.ds(lo, n), :] if kind == "a" else place
        at = u * 8 + "abcd".index(kind) * 2 + (0 if sign > 0 else 1)
        return pltpu.make_async_remote_copy(
            src_ref=source,
            dst_ref=place,
            send_sem=zsend.at[at],
            recv_sem=zrecv.at[at],
            device_id=device(sign * near, 0),
            device_id_type=MESH,
        )

    for u in range(6):
        for dy in (1, 3, 2):
            ycopy(u, dy, y).start()
    for m in range(3):
        for h, (lo, n) in enumerate(PARTS):
            ybufs[h][m, :, pl.ds(y * rows, rows), :] = sources[m][:, y, :, lo : lo + n]

    def turn(u):
        m, h = units[u]
        lo, n = PARTS[h]
        for dy in (1, 3, 2):
            ycopy(u, dy, yat(-dy)).wait_recv()
        away[m, pl.ds(lo, n), :] = ybufs[h][m, 1 - parity].T
        outs[m][z, pl.ds(lo, n), :] = ybufs[h][m, parity].T

    def first(u):
        turn(u)
        for kind in "ab":
            for sign in (1, -1):
                zcopy(u, kind, sign).start()

    def second(u):
        for kind, after in (("a", "c"), ("b", "d")):
            for sign in (1, -1):
                zcopy(u, kind, sign, True).wait_recv()
                zcopy(u, after, sign).start()

    first(0)
    for u in range(6):
        if u < 5:
            first(u + 1)
        second(u)
    for u in range(6):
        for kind in "cd":
            for sign in (1, -1):
                zcopy(u, kind, sign, True).wait_recv()
    for u in range(6):
        for dy in (1, 3, 2):
            ycopy(u, dy, y).wait_send()
        for kind in "abcd":
            for sign in (1, -1):
                zcopy(u, kind, sign).wait_send()


def handed_over(gate, up, down):
    _, rows, width = gate.shape
    split = [w.reshape(2, NY, rows, width) for w in (gate, up, down)]
    out = jax.ShapeDtypeStruct((NZ, width, NY * rows), jnp.bfloat16)
    dma = pltpu.SemaphoreType.DMA
    return pl.pallas_call(
        weights_kernel,
        out_shape=(out, out, out),
        in_specs=[pl.BlockSpec(memory_space=pltpu.VMEM)] * 3,
        out_specs=(pl.BlockSpec(memory_space=pltpu.VMEM),) * 3,
        scratch_shapes=[
            pltpu.VMEM((3, 2, NY * rows, PARTS[0][1]), jnp.bfloat16),
            pltpu.VMEM((3, 2, NY * rows, PARTS[1][1]), jnp.bfloat16),
            pltpu.VMEM((3, width, NY * rows), jnp.bfloat16),
            dma((18,)),
            dma((18,)),
            dma((48,)),
            dma((48,)),
        ],
        compiler_params=pltpu.CompilerParams(
            collective_id=0, has_side_effects=True, vmem_limit_bytes=40 * 1024 * 1024
        ),
        cost_estimate=pl.CostEstimate(flops=10**11, bytes_accessed=10**7, transcendentals=0),
    )(*split)


def slot_plan(routes, most):
    experts_all = jnp.arange(EXPERTS, dtype=jnp.int32)
    named = (routes.T[:, None, :] == experts_all[None, :, None]).astype(jnp.bfloat16)
    tokens = routes.shape[0]
    places = jnp.arange(tokens)
    before = (places[:, None] < places[None, :]).astype(jnp.bfloat16)
    rank = jnp.dot(named.reshape(-1, tokens), before, preferred_element_type=jnp.float32)
    rank = rank.reshape(named.shape)
    count = jnp.sum(named[0].astype(jnp.float32), axis=1)
    rank = rank + jnp.stack([jnp.zeros_like(count), count])[:, :, None]
    slot = rank + most * experts_all[None, :, None].astype(jnp.float32)
    return jnp.sum(jnp.where(named > 0, slot, 0.0), axis=1).astype(jnp.int32)


def shards(tokens, norm_gain, gate_train, up_train, down_train, routes, route_logits):
    fs_count = lax.axis_size("fs")
    groups = [list(range(at, at + EXPERTS)) for at in range(0, fs_count, EXPERTS)]
    tok_rows, features = tokens.shape
    most = tok_rows // 2
    gain_rows = norm_gain[None, :, None]
    gate_low = (gate_train.astype(jnp.float32) * gain_rows).astype(jnp.bfloat16)
    up_low = (up_train.astype(jnp.float32) * gain_rows).astype(jnp.bfloat16)

    slots = slot_plan(routes, most)
    slot_ids = jnp.arange(EXPERTS * most, dtype=jnp.int32)
    chosen = [(slots[k][None, :] == slot_ids[:, None]).astype(jnp.bfloat16) for k in range(2)]
    outgoing = jnp.dot(chosen[0] + chosen[1], tokens, preferred_element_type=jnp.float32)
    outgoing = outgoing.astype(jnp.bfloat16).reshape(EXPERTS, most, features)
    arrived = lax.all_to_all(
        outgoing, "fs", split_axis=0, concat_axis=0, tiled=True, axis_index_groups=groups
    )
    arrived = arrived.reshape(EXPERTS * most, features)
    arrived, gate_low, up_low, down_low = lax.optimization_barrier(
        (arrived, gate_low, up_low, down_train)
    )
    handed = handed_over(gate_low, up_low, down_low)
    gate_out, up_out, down_out = (
        w.transpose(0, 2, 1).reshape(1, -1, gate_train.shape[2]) for w in handed
    )
    arrived = lax.all_gather(arrived, "tp", axis=1, tiled=True)
    arrived_float = arrived.astype(jnp.float32)
    inverse = lax.rsqrt(jnp.mean(arrived_float * arrived_float, axis=1, keepdims=True) + epsilon)
    normed = (arrived_float * inverse).astype(jnp.bfloat16)
    gate_val = jnp.dot(normed, gate_out[0], preferred_element_type=jnp.float32)
    up_val = jnp.dot(normed, up_out[0], preferred_element_type=jnp.float32)
    active = (jax.nn.silu(gate_val) * up_val).astype(jnp.bfloat16)
    summed = lax.psum_scatter(
        lax.dot_general(
            active, down_out[0], (((1,), (1,)), ((), ())), preferred_element_type=jnp.float32
        ).astype(jnp.bfloat16),
        "tp",
        scatter_dimension=1,
        tiled=True,
    )
    returned = lax.all_to_all(
        summed.reshape(EXPERTS, most, features),
        "fs",
        split_axis=0,
        concat_axis=0,
        tiled=True,
        axis_index_groups=groups,
    ).reshape(EXPERTS * most, features)
    picked = [
        lax.dot_general(
            c, returned, (((0,), (0,)), ((), ())), preferred_element_type=jnp.float32
        )
        for c in chosen
    ]
    first = jax.nn.sigmoid(route_logits[:, 0] - route_logits[:, 1])
    second = jax.nn.sigmoid(route_logits[:, 1] - route_logits[:, 0])
    mixed = picked[0] * first[:, None] + picked[1] * second[:, None]
    return (gate_out, up_out, down_out, mixed.astype(jnp.bfloat16))


def solution(mesh):
    placed = (
        P("fs", "tp"),
        P("fs"),
        P(None, "fs", "tp"),
        P(None, "fs", "tp"),
        P(None, "fs", "tp"),
        P("fs", None),
        P("fs", None),
    )
    return jax.shard_map(
        shards,
        mesh=mesh,
        in_specs=placed,
        out_specs=(P("fs", None, "tp"), P("fs", None, "tp"), P("fs", None, "tp"), P("fs", "tp")),
        check_vma=False,
    )
```

```python
import functools

import jax
import jax.numpy as jnp
from jax import lax
from jax.experimental import pallas as pl
from jax.experimental.pallas import tpu as pltpu
from jax.sharding import PartitionSpec as P

EXPERTS = 8
epsilon = 1e-06
MESH = pl.DeviceIdType.MESH
NZ, NY = 8, 4
VMEM_LIMIT = 54 * 1024 * 1024
PARTS = ((0, 384), (384, 320))


NX = 4
COLS = (((1,), (0,)), ((), ()))
ROWS = (((1,), (1,)), ((), ()))


def whole_kernel(
    g_ref, u_ref, d_ref, gain_ref, tok_ref, row_ref, col_ref, logit_ref,
    og, ou, od, mix_ref,
    scaled, y0, y1, away, xs, xall, inv_ref, hidden, theirs, got, mine, joint, parts, ret, back,
    ysend, yrecv, zsend, zrecv, tsend, trecv, asend, arecv, psend, precv, rsend, rrecv, bsend, brecv,
):
    fs = lax.axis_index("fs")
    tp = lax.axis_index("tp")
    z, y = fs // NY, lax.rem(fs, NY)
    x, core = tp // 2, lax.rem(tp, 2)
    parity = lax.rem(z, 2)
    sources, outs, ybufs = (scaled.at[0], scaled.at[1], d_ref), (og, ou, od), (y0, y1)
    rows = g_ref.shape[2]
    most = xs.shape[1]
    slots = xall.shape[1]
    half_slots = slots // 2
    here = parity * NY + y

    def zat(step):
        return lax.rem(z + step + NZ, NZ)

    def yat(step):
        return lax.rem(y + step + NY, NY)

    def device(dz, dy):
        return {"fs": zat(dz) * NY + yat(dy)}

    def member(flip, dy):
        p = (1 - parity) if flip else parity
        return (z - parity + p) * NY + yat(dy), p * NY + yat(dy)

    def mate(step):
        return {"tp": lax.rem(x + step + NX, NX) * 2 + core}

    partner = {"tp": x * 2 + 1 - core}

    group = [(0, 1), (0, 3), (0, 2), (1, 0), (1, 1), (1, 3), (1, 2)]
    barrier = pltpu.get_barrier_semaphore()
    greeted = [device(0, 1), device(0, 2), device(0, 3)]
    greeted += [device(1, 0), device(-1, 0), device(2, 0), device(-2, 0)]
    greeted += [{"fs": member(1, dy)[0]} for dy in (1, 2, 3)]
    greeted += [{"tp": lax.rem(tp + step, 2 * NX)} for step in range(1, 2 * NX)]
    for other in greeted:
        pl.semaphore_signal(barrier, inc=1, device_id=other, device_id_type=MESH)
    pl.semaphore_wait(barrier, len(greeted))

    units = [(m, h) for m in range(3) for h in range(2)]

    def ycopy(u, dy, to_row):
        m, h = units[u]
        lo, n = PARTS[h]
        return pltpu.make_async_remote_copy(
            src_ref=sources[m].at[:, yat(dy), :, pl.ds(lo, n)],
            dst_ref=ybufs[h].at[m, :, pl.ds(to_row * rows, rows), :],
            send_sem=ysend.at[u * 3 + dy - 1],
            recv_sem=yrecv.at[u * 3 + dy - 1],
            device_id=device(0, dy),
            device_id_type=MESH,
        )

    def zcopy(u, kind, sign, arriving=False):
        m, h = units[u]
        lo, n = PARTS[h]
        out = outs[m]
        near = {"a": 1, "b": 2, "c": 2, "d": 2}[kind]
        hops = {"a": 0, "b": 0, "c": 1, "d": 2}[kind]
        block = zat(-sign * hops)
        if arriving:
            block = zat(-sign * (hops + near))
        if kind == "d":
            half = n // 2
            lo, n = (lo, half) if sign > 0 else (lo + half, half)
        place = out.at[block, pl.ds(lo, n), :]
        source = away.at[m, pl.ds(lo, n), :] if kind == "a" else place
        at = u * 8 + "abcd".index(kind) * 2 + (0 if sign > 0 else 1)
        return pltpu.make_async_remote_copy(
            src_ref=source,
            dst_ref=place,
            send_sem=zsend.at[at],
            recv_sem=zrecv.at[at],
            device_id=device(sign * near, 0),
            device_id_type=MESH,
        )

    def tokens_copy(flip, dy, arriving=False):
        to, expert = member(flip, dy)
        owner = member(flip, -dy)[1] if arriving else here
        at = flip * NY + dy
        return pltpu.make_async_remote_copy(
            src_ref=xs.at[expert],
            dst_ref=xall.at[tp, pl.ds(pl.multiple_of(owner * most, 16), most), :],
            send_sem=tsend.at[at],
            recv_sem=trecv.at[at],
            device_id={"fs": to},
            device_id_type=MESH,
        )

    def gather_copy(step, arriving=False):
        block = lax.rem(x - step + NX, NX) * 2 + core if arriving else tp
        return pltpu.make_async_remote_copy(
            src_ref=xall.at[tp],
            dst_ref=xall.at[block],
            send_sem=asend.at[step],
            recv_sem=arecv.at[step],
            device_id=mate(step),
            device_id_type=MESH,
        )

    def relay_copy(step, arriving=False):
        block = lax.rem(x - step + NX, NX) * 2 + core
        if arriving:
            block = lax.rem(x - step + NX, NX) * 2 + 1 - core
        return pltpu.make_async_remote_copy(
            src_ref=xall.at[block],
            dst_ref=xall.at[block],
            send_sem=asend.at[NX + step],
            recv_sem=arecv.at[NX + step],
            device_id=partner,
            device_id_type=MESH,
        )

    def block_at(k):
        return lax.rem(z + (2 * lax.rem(k, 2) - 1) * ((k + 1) // 2) + NZ, NZ)

    def pair_copy(k):
        return pltpu.make_async_remote_copy(
            src_ref=theirs.at[k],
            dst_ref=got.at[k],
            send_sem=psend.at[k],
            recv_sem=precv.at[k],
            device_id=partner,
            device_id_type=MESH,
        )

    def half_rows(which):
        return pl.ds(pl.multiple_of(which * half_slots, 16), half_slots)

    def sum_copy(k, to, sender):
        return pltpu.make_async_remote_copy(
            src_ref=joint.at[k],
            dst_ref=parts.at[sender // 2, half_rows(lax.rem(sender, 2)), :],
            send_sem=rsend.at[k],
            recv_sem=rrecv.at[sender],
            device_id={"tp": to},
            device_id_type=MESH,
        )

    def back_copy(flip, dy, arriving=False):
        to, owner = member(flip, dy)
        expert = member(flip, -dy)[1] if arriving else here
        at = flip * NY + dy
        return pltpu.make_async_remote_copy(
            src_ref=ret.at[owner],
            dst_ref=back.at[expert],
            send_sem=bsend.at[at],
            recv_sem=brecv.at[at],
            device_id={"fs": to},
            device_id_type=MESH,
        )

    def scale(m, ref):
        gain = gain_ref[...]

        def one(e, carry):
            block = ref[e // NY, lax.rem(e, NY)]
            scaled[m, e // NY, lax.rem(e, NY)] = (block.astype(jnp.float32) * gain).astype(
                jnp.bfloat16
            )
            return carry

        lax.fori_loop(0, EXPERTS, one, 0)

    def across(m):
        for u in (2 * m, 2 * m + 1):
            for dy in (1, 3, 2):
                ycopy(u, dy, y).start()
        for h, (lo, n) in enumerate(PARTS):
            ybufs[h][m, :, pl.ds(y * rows, rows), :] = sources[m][:, y, :, lo : lo + n]

    scale(0, g_ref)
    across(0)

    def pick(e, carry):
        ids = lax.broadcasted_iota(jnp.int32, (most, tok_ref.shape[0]), 0) + e * most
        hit = (ids == row_ref[0:1, :]) | (ids == row_ref[1:2, :])
        chosen = jnp.where(hit, 1.0, 0.0).astype(jnp.bfloat16)
        xs[e] = jnp.dot(chosen, tok_ref[...], preferred_element_type=jnp.float32).astype(
            jnp.bfloat16
        )
        return carry

    lax.fori_loop(0, EXPERTS, pick, 0)
    for flip, dy in group:
        tokens_copy(flip, dy).start()
    xall[tp, pl.ds(pl.multiple_of(here * most, 16), most), :] = xs[here]
    scale(1, u_ref)
    across(1)
    across(2)

    def turn(u):
        m, h = units[u]
        lo, n = PARTS[h]
        for dy in (1, 3, 2):
            ycopy(u, dy, yat(-dy)).wait_recv()
        away[m, pl.ds(lo, n), :] = ybufs[h][m, 1 - parity].T
        outs[m][z, pl.ds(lo, n), :] = ybufs[h][m, parity].T

    def first(u):
        turn(u)
        for kind in "ab":
            for sign in (1, -1):
                zcopy(u, kind, sign).start()

    def second(u):
        for kind, after in (("a", "c"), ("b", "d")):
            for sign in (1, -1):
                zcopy(u, kind, sign, True).wait_recv()
                zcopy(u, after, sign).start()

    def landed(u):
        for kind in "cd":
            for sign in (1, -1):
                zcopy(u, kind, sign, True).wait_recv()

    first(0)
    first(1)
    for flip, dy in group:
        tokens_copy(flip, dy, True).wait_recv()
    for step in (1, 3, 2):
        gather_copy(step).start()
    relay_copy(0).start()
    second(0)
    first(2)
    second(1)
    first(3)
    for step in (1, 3):
        gather_copy(step, True).wait_recv()
        relay_copy(step).start()
    second(2)
    first(4)
    gather_copy(2, True).wait_recv()
    relay_copy(2).start()
    second(3)
    first(5)
    second(4)
    for step in range(NX):
        relay_copy(step, True).wait_recv()

    def norms(i, carry):
        at = pl.ds(pl.multiple_of(i * most, 16), most)
        total = jnp.zeros((most, 1), jnp.float32)
        for block in range(xall.shape[0]):
            v = xall[block, at, :].astype(jnp.float32)
            total = total + jnp.sum(v * v, axis=1, keepdims=True)
        mean = total / (xall.shape[0] * xall.shape[2])
        inv_ref[at, :] = lax.rsqrt(mean + epsilon)
        return carry

    lax.fori_loop(0, EXPERTS, norms, 0)
    for u in range(4):
        landed(u)

    tile = slots // 4

    def hide(i, carry):
        at = pl.ds(pl.multiple_of(i * tile, 16), tile)
        gate = jnp.zeros((tile, og.shape[1]), jnp.float32)
        up = jnp.zeros((tile, og.shape[1]), jnp.float32)
        for block in range(NZ):
            v = xall[block, at, :]
            gate = gate + lax.dot_general(v, og[block], ROWS, preferred_element_type=jnp.float32)
            up = up + lax.dot_general(v, ou[block], ROWS, preferred_element_type=jnp.float32)
        inverse = inv_ref[at, :]
        gate = gate * inverse
        up = up * inverse
        hidden[at, :] = (gate / (1.0 + jnp.exp(-gate)) * up).astype(jnp.bfloat16)
        return carry

    lax.fori_loop(0, slots // tile, hide, 0)
    second(5)

    def project(k, carry):
        weights = od[block_at(k)]
        theirs[k] = lax.dot_general(
            hidden[half_rows(1 - core), :], weights, COLS, preferred_element_type=jnp.float32
        ).astype(jnp.bfloat16)
        pair_copy(k).start()
        mine[k] = lax.dot_general(
            hidden[half_rows(core), :], weights, COLS, preferred_element_type=jnp.float32
        ).astype(jnp.bfloat16)
        return carry

    def join(k, carry):
        to = block_at(k)
        pair_copy(k).wait_recv()
        joint[k] = (mine[k].astype(jnp.float32) + got[k].astype(jnp.float32)).astype(jnp.bfloat16)

        @pl.when(to != tp)
        def _():
            sum_copy(k, to, tp).start()

        @pl.when(to == tp)
        def _():
            parts[x, half_rows(core), :] = joint[k]

        return carry

    lax.fori_loop(0, 5, project, 0)
    lax.fori_loop(0, 5, join, 0)
    landed(4)
    landed(5)
    lax.fori_loop(5, NZ, project, 0)
    lax.fori_loop(5, NZ, join, 0)

    for step in range(1, 2 * NX):
        sender = lax.rem(tp + step, 2 * NX)
        sum_copy(0, sender, sender).wait_recv()

    def total(owner):
        at = pl.ds(pl.multiple_of(owner * most, 16), most)
        value = parts[0, at, :].astype(jnp.float32)
        for block in range(1, NX):
            value = value + parts[block, at, :].astype(jnp.float32)
        ret[owner] = value.astype(jnp.bfloat16)

    for flip, dy in group:
        total(member(flip, dy)[1])
        back_copy(flip, dy).start()
    total(here)
    back[here] = ret[here]
    for flip, dy in group:
        back_copy(flip, dy, True).wait_recv()

    count = tok_ref.shape[0]
    piece = count // 3

    def mix(i, carry):
        at = pl.ds(pl.multiple_of(i * piece, 16), piece)
        ids = lax.broadcasted_iota(jnp.int32, (piece, slots), 1)
        results = back[...].reshape(slots, back.shape[2])
        wanted = col_ref[at, :]
        scores = logit_ref[at, :]
        value = jnp.zeros((piece, back.shape[2]), jnp.float32)
        for k in range(2):
            chosen = jnp.where(ids == wanted[:, k : k + 1], 1.0, 0.0).astype(jnp.bfloat16)
            picked = jnp.dot(chosen, results, preferred_element_type=jnp.float32)
            value = value + picked * jax.nn.sigmoid(
                scores[:, k : k + 1] - scores[:, 1 - k : 2 - k]
            )
        mix_ref[at, :] = value.astype(jnp.bfloat16)
        return carry

    lax.fori_loop(0, count // piece, mix, 0)

    for u in range(6):
        for dy in (1, 3, 2):
            ycopy(u, dy, y).wait_send()
        for kind in "abcd":
            for sign in (1, -1):
                zcopy(u, kind, sign).wait_send()
    for flip, dy in group:
        tokens_copy(flip, dy).wait_send()
        back_copy(flip, dy).wait_send()
    for step in range(1, NX):
        gather_copy(step).wait_send()
    for step in range(NX):
        relay_copy(step).wait_send()

    def sent(k, carry):
        pair_copy(k).wait_send()
        to = block_at(k)

        @pl.when(to != tp)
        def _():
            sum_copy(k, to, tp).wait_send()

        return carry

    lax.fori_loop(0, NZ, sent, 0)


def whole(gate, up, down, gain, tokens, slots, logits):
    _, rows, width = gate.shape
    count, features = tokens.shape
    most = count // 2
    split = [w.reshape(2, NY, rows, width) for w in (gate, up, down)]
    out = jax.ShapeDtypeStruct((NZ, width, NY * rows), jnp.bfloat16)
    dma = pltpu.SemaphoreType.DMA
    vmem = lambda *shape, dtype=jnp.bfloat16: pltpu.VMEM(shape, dtype)
    total = EXPERTS * most
    return pl.pallas_call(
        whole_kernel,
        out_shape=(out, out, out, jax.ShapeDtypeStruct((count, features), jnp.bfloat16)),
        in_specs=[pl.BlockSpec(memory_space=pltpu.VMEM)] * 8,
        out_specs=(pl.BlockSpec(memory_space=pltpu.VMEM),) * 4,
        scratch_shapes=[
            vmem(2, 2, NY, rows, width),
            vmem(3, 2, NY * rows, PARTS[0][1]),
            vmem(3, 2, NY * rows, PARTS[1][1]),
            vmem(3, width, NY * rows),
            vmem(EXPERTS, most, features),
            vmem(2 * NX, total, features),
            vmem(total, 1, dtype=jnp.float32),
            vmem(total, width),
            vmem(NZ, total // 2, features),
            vmem(NZ, total // 2, features),
            vmem(NZ, total // 2, features),
            vmem(NZ, total // 2, features),
            vmem(NX, total, features),
            vmem(EXPERTS, most, features),
            vmem(EXPERTS, most, features),
            dma((18,)), dma((18,)), dma((48,)), dma((48,)), dma((8,)), dma((8,)), dma((8,)), dma((8,)),
            dma((8,)), dma((8,)), dma((8,)), dma((8,)), dma((8,)), dma((8,)),
        ],
        compiler_params=pltpu.CompilerParams(
            collective_id=0, has_side_effects=True, vmem_limit_bytes=VMEM_LIMIT
        ),
        cost_estimate=pl.CostEstimate(flops=10**11, bytes_accessed=10**7, transcendentals=0),
    )(*split, gain, tokens, slots, slots.T, logits)


def place_kernel(g_ref, u_ref, d_ref, og, ou, od, sem):
    copies = []
    for m, (ref, out) in enumerate(((g_ref, og), (u_ref, ou), (d_ref, od))):
        for block in range(NZ):
            size = ref.shape[2]
            copies.append(
                pltpu.make_async_copy(
                    ref.at[block], out.at[:, pl.ds(block * size, size)], sem.at[m * NZ + block]
                )
            )
    for copy in copies:
        copy.start()
    for copy in copies:
        copy.wait()


def placed_out(blocks):
    nz, width, size = blocks[0].shape
    out = jax.ShapeDtypeStruct((width, nz * size), jnp.bfloat16)
    done = pl.pallas_call(
        place_kernel,
        out_shape=(out,) * 3,
        in_specs=[pl.BlockSpec(memory_space=pltpu.VMEM)] * 3,
        out_specs=(pl.BlockSpec(memory_space=pl.ANY),) * 3,
        scratch_shapes=[pltpu.SemaphoreType.DMA((3 * NZ,))],
    )(*blocks)
    return [o.T[None] for o in done]


def slot_plan(routes, most):
    experts_all = jnp.arange(EXPERTS, dtype=jnp.int32)
    named = (routes.T[:, None, :] == experts_all[None, :, None]).astype(jnp.bfloat16)
    tokens = routes.shape[0]
    places = jnp.arange(tokens)
    before = (places[:, None] < places[None, :]).astype(jnp.bfloat16)
    rank = jnp.dot(named.reshape(-1, tokens), before, preferred_element_type=jnp.float32)
    rank = rank.reshape(named.shape)
    count = jnp.sum(named[0].astype(jnp.float32), axis=1)
    rank = rank + jnp.stack([jnp.zeros_like(count), count])[:, :, None]
    slot = rank + most * experts_all[None, :, None].astype(jnp.float32)
    return jnp.sum(jnp.where(named > 0, slot, 0.0), axis=1).astype(jnp.int32)


def shards(tokens, norm_gain, gate_train, up_train, down_train, routes, route_logits):
    slots = slot_plan(routes, tokens.shape[0] // 2)
    *blocks, mixed = whole(
        gate_train, up_train, down_train, norm_gain[:, None], tokens, slots, route_logits
    )
    return (*placed_out(blocks), mixed)


def solution(mesh):
    placed = (
        P("fs", "tp"),
        P("fs"),
        P(None, "fs", "tp"),
        P(None, "fs", "tp"),
        P(None, "fs", "tp"),
        P("fs", None),
        P("fs", None),
    )
    return jax.shard_map(
        shards,
        mesh=mesh,
        in_specs=placed,
        out_specs=(P("fs", None, "tp"), P("fs", None, "tp"), P("fs", None, "tp"), P("fs", "tp")),
        check_vma=False,
    )
```

```python
import functools

import jax
import jax.numpy as jnp
from jax import lax
from jax.experimental import pallas as pl
from jax.experimental.pallas import tpu as pltpu
from jax.sharding import PartitionSpec as P

EXPERTS = 8
epsilon = 1e-06
MESH = pl.DeviceIdType.MESH
NZ, NY = 8, 4
VMEM_LIMIT = 60 * 1024 * 1024
NZ, NY, NX = 8, 4, 4
LANES = 128
SPLIT = ((0, 0, 128), (0, 128, 256), (0, 384, 320), (1, 0, 384), (1, 384, 320))
DOWN = ((2, 0, 384), (2, 384, 320))
ACROSS = SPLIT + DOWN
UNITS = len(SPLIT) + 2
COLS = (((1,), (0,)), ((), ()))
ROWS = (((1,), (1,)), ((), ()))
FULL = 5


def whole_kernel(
    g_in, u_in, d_in, gain_in, tok_in, route_in, logit_in,
    g_out, u_out, d_out, mix_ref,
    og, ou, od, g_ref, u_ref, d_ref, gain_ref, tok_ref, route_ref, logit_ref, scaled, ybuf, away, awayd, slot_ref, xs, xall, inv_ref, hidden,
    theirs, got, mine, joint, far, theirs_h, got_h, mine_h, joint_h, far_h, parts, ret, back,
    ysend, yrecv, zsend, zrecv, tsend, trecv, asend, arecv, psend, precv, fsend, frecv, rrecv, bsend, brecv, lsem, osem,
):
    fs = lax.axis_index("fs")
    tp = lax.axis_index("tp")
    z, y = fs // NY, lax.rem(fs, NY)
    x, core = tp // 2, lax.rem(tp, 2)
    parity = lax.rem(z, 2)
    sources = (scaled.at[0], scaled.at[1], d_ref)
    rows = g_ref.shape[2]
    width = g_ref.shape[3]
    most = xs.shape[1]
    few = most // 2
    slots = xall.shape[1]
    half_slots = slots // 2
    quarter = slots // 4
    here = parity * NY + y

    def zat(step):
        return lax.rem(z + step + NZ, NZ)

    def yat(step):
        return lax.rem(y + step + NY, NY)

    def device(dz, dy):
        return {"fs": zat(dz) * NY + yat(dy)}

    def mate(step):
        return {"tp": lax.rem(x + step + NX, NX) * 2 + core}

    partner = {"tp": x * 2 + 1 - core}
    group = [(dz, dy) for dz, dys in ((1, (0, 1, 3, 2)), (-1, (0, 1, 3, 2)), (0, (1, 3, 2))) for dy in dys]

    loads = [
        pltpu.make_async_copy(source, held, lsem.at[i])
        for i, (source, held) in enumerate(
            (
                (g_in, g_ref),
                (gain_in, gain_ref),
                (route_in, route_ref),
                (tok_in, tok_ref),
                (u_in, u_ref),
                (d_in, d_ref),
                (logit_in, logit_ref),
            )
        )
    ]
    for load in loads:
        load.start()
    barrier = pltpu.get_barrier_semaphore()
    greeted = [device(dz, dy) for dz, dy in group + [(2, 0), (-2, 0)]]
    greeted += [{"tp": lax.rem(tp + step, 2 * NX)} for step in range(1, 2 * NX)]
    for other in greeted:
        pl.semaphore_signal(barrier, inc=1, device_id=other, device_id_type=MESH)
    pl.semaphore_wait(barrier, len(greeted))

    def ycopy(u, dy, to_row):
        m, lo, n = ACROSS[u]
        return pltpu.make_async_remote_copy(
            src_ref=sources[m].at[:, yat(dy), :, pl.ds(lo, n)],
            dst_ref=ybuf.at[m, :, pl.ds(to_row * rows, rows), pl.ds(lo, n)],
            send_sem=ysend.at[u * 3 + dy - 1],
            recv_sem=yrecv.at[u * 3 + dy - 1],
            device_id=device(0, dy),
            device_id_type=MESH,
        )

    def zcopy(u, kind, sign, arriving=False):
        if u < len(SPLIT):
            m, lo, n = SPLIT[u]
            out, left = (og, ou)[m], away.at[m]
        else:
            lo, n = 0, width
            out, left = od.at[u - len(SPLIT)], awayd.at[u - len(SPLIT)]
        near = {"a": 1, "b": 2, "c": 2, "d": 2}[kind]
        hops = {"a": 0, "b": 0, "c": 1, "d": 2}[kind]
        block = zat(-sign * hops)
        if arriving:
            block = zat(-sign * (hops + near))
        if kind == "d":
            half = n // 2
            lo, n = (lo, half) if sign > 0 else (lo + half, half)
        place = out.at[block, pl.ds(lo, n), :]
        source = left.at[pl.ds(lo, n), :] if kind == "a" else place
        at = u * 8 + "abcd".index(kind) * 2 + (0 if sign > 0 else 1)
        return pltpu.make_async_remote_copy(
            src_ref=source,
            dst_ref=place,
            send_sem=zsend.at[at],
            recv_sem=zrecv.at[at],
            device_id=device(sign * near, 0),
            device_id_type=MESH,
        )

    def base(dz):
        return {0: 0, 1: half_slots, -1: half_slots + quarter}[dz]

    def arrived_rows(dz, at_y):
        n = few if dz else most
        return pl.ds(pl.multiple_of(base(dz) + at_y * n, 16), n)

    def held_rows(dz):
        return pl.ds({0: 0, 1: 0, -1: few}[dz], few if dz else most)

    def expert(dz, at_y):
        return ((1 - parity) if dz else parity) * NY + at_y

    def tokens_copy(dz, dy, arriving=False):
        at = (dz + 1) * NY + dy
        return pltpu.make_async_remote_copy(
            src_ref=xs.at[expert(dz, yat(dy)), held_rows(dz), :],
            dst_ref=xall.at[tp, arrived_rows(dz, yat(-dy) if arriving else y), :],
            send_sem=tsend.at[at],
            recv_sem=trecv.at[at],
            device_id=device(dz, dy),
            device_id_type=MESH,
        )

    def back_copy(dz, dy, arriving=False):
        at = (dz + 1) * NY + dy
        owner = expert(dz, yat(-dy)) if arriving else here
        return pltpu.make_async_remote_copy(
            src_ref=ret.at[arrived_rows(dz, yat(dy)), :],
            dst_ref=back.at[owner, held_rows(dz), :],
            send_sem=bsend.at[at],
            recv_sem=brecv.at[at],
            device_id=device(-dz, dy),
            device_id_type=MESH,
        )

    def gather_copy(step, arriving=False):
        block = lax.rem(x - step + NX, NX) * 2 + core if arriving else tp
        return pltpu.make_async_remote_copy(
            src_ref=xall.at[tp],
            dst_ref=xall.at[block],
            send_sem=asend.at[step],
            recv_sem=arecv.at[step],
            device_id=mate(step),
            device_id_type=MESH,
        )

    def relay_copy(step, arriving=False):
        block = lax.rem(x - step + NX, NX) * 2 + core
        if arriving:
            block = lax.rem(x - step + NX, NX) * 2 + 1 - core
        return pltpu.make_async_remote_copy(
            src_ref=xall.at[block],
            dst_ref=xall.at[block],
            send_sem=asend.at[NX + step],
            recv_sem=arecv.at[NX + step],
            device_id=partner,
            device_id_type=MESH,
        )

    def scale(m, ref):
        wide = gain_ref[...]
        on = lax.broadcasted_iota(jnp.int32, (rows, rows), 0) == lax.broadcasted_iota(
            jnp.int32, (rows, rows), 1
        )
        gain = jnp.sum(jnp.where(on, wide, 0.0), axis=1, keepdims=True)

        def one(e, carry):
            block = ref[e // NY, lax.rem(e, NY)]
            scaled[m, e // NY, lax.rem(e, NY)] = (block.astype(jnp.float32) * gain).astype(
                jnp.bfloat16
            )
            return carry

        lax.fori_loop(0, EXPERTS, one, 0)

    def across(m):
        for u, (owner, lo, n) in enumerate(ACROSS):
            if owner == m:
                for dy in (1, 3, 2):
                    ycopy(u, dy, y).start()
        ybuf[m, :, pl.ds(y * rows, rows), :] = sources[m][:, y]

    def plan():
        count = tok_ref.shape[0]
        lines = lax.broadcasted_iota(jnp.int32, (2 * EXPERTS, count), 0)
        routes = route_ref[...]
        named = (routes[0:1, :] == lines) | (routes[1:2, :] == lines - EXPERTS)
        named = jnp.where(named, 1.0, 0.0)
        before = jnp.where(
            lax.broadcasted_iota(jnp.int32, (count, count), 0)
            < lax.broadcasted_iota(jnp.int32, (count, count), 1),
            1.0,
            0.0,
        )
        rank = jnp.dot(
            named.astype(jnp.bfloat16),
            before.astype(jnp.bfloat16),
            preferred_element_type=jnp.float32,
        )
        for k in range(2):
            one = named[k * EXPERTS : (k + 1) * EXPERTS]
            place = rank[k * EXPERTS : (k + 1) * EXPERTS]
            if k:
                place = place + jnp.sum(named[:EXPERTS], axis=1, keepdims=True)
            place = place + (lines[:EXPERTS] * most).astype(jnp.float32)
            slot = jnp.sum(one * place, axis=0, keepdims=True)
            slot_ref[k : k + 1, :] = slot.astype(jnp.int32)

    for load in loads[:2]:
        load.wait()
    scale(0, g_ref)
    across(0)
    for load in loads[2:]:
        load.wait()
    plan()

    def pick(e, carry):
        ids = lax.broadcasted_iota(jnp.int32, (most, tok_ref.shape[0]), 0) + e * most
        hit = (ids == slot_ref[0:1, :]) | (ids == slot_ref[1:2, :])
        chosen = jnp.where(hit, 1.0, 0.0).astype(jnp.bfloat16)
        xs[e] = jnp.dot(chosen, tok_ref[...], preferred_element_type=jnp.float32).astype(
            jnp.bfloat16
        )
        return carry

    lax.fori_loop(0, EXPERTS, pick, 0)
    for dz, dy in group:
        tokens_copy(dz, dy).start()
    xall[tp, arrived_rows(0, y), :] = xs[here]
    scale(1, u_ref)
    across(1)
    across(2)

    def turn(u):
        if u < len(SPLIT):
            m, lo, n = SPLIT[u]
            for dy in (1, 3, 2):
                ycopy(u, dy, yat(-dy)).wait_recv()
            away[m, pl.ds(lo, n), :] = ybuf[m, 1 - parity, :, lo : lo + n].T
            (og, ou)[m][z, pl.ds(lo, n), :] = ybuf[m, parity, :, lo : lo + n].T
        elif u == len(SPLIT):
            for part, (m, lo, n) in enumerate(DOWN):
                for dy in (1, 3, 2):
                    ycopy(u + part, dy, yat(-dy)).wait_recv()
                gone = ybuf[m, 1 - parity, :, lo : lo + n].T
                kept = ybuf[m, parity, :, lo : lo + n].T
                for f in range(2):
                    awayd[f, pl.ds(lo, n), :] = gone[:, f * LANES : (f + 1) * LANES]
                    od[f, z, pl.ds(lo, n), :] = kept[:, f * LANES : (f + 1) * LANES]

    def first(u):
        turn(u)
        for kind in "ab":
            for sign in (1, -1):
                zcopy(u, kind, sign).start()

    def second(u):
        for kind, after in (("a", "c"), ("b", "d")):
            for sign in (1, -1):
                zcopy(u, kind, sign, True).wait_recv()
                zcopy(u, after, sign).start()

    def landed(u):
        for kind in "cd":
            for sign in (1, -1):
                zcopy(u, kind, sign, True).wait_recv()

    first(0)
    first(1)
    second(0)
    for dz, dy in group:
        tokens_copy(dz, dy, True).wait_recv()
    for step in (1, 3, 2):
        gather_copy(step).start()
    relay_copy(0).start()
    first(2)
    second(1)
    first(3)
    second(2)
    first(4)
    for step in (1, 3):
        gather_copy(step, True).wait_recv()
        relay_copy(step).start()
    second(3)
    first(5)
    gather_copy(2, True).wait_recv()
    relay_copy(2).start()
    second(4)
    first(6)
    second(5)
    for step in range(NX):
        relay_copy(step, True).wait_recv()

    def norms(i, carry):
        at = pl.ds(pl.multiple_of(i * most, 16), most)
        total = jnp.zeros((most, 1), jnp.float32)
        for block in range(xall.shape[0]):
            v = xall[block, at, :].astype(jnp.float32)
            total = total + jnp.sum(v * v, axis=1, keepdims=True)
        mean = total / (xall.shape[0] * xall.shape[2])
        inv_ref[at, :] = lax.rsqrt(mean + epsilon)
        return carry

    lax.fori_loop(0, EXPERTS, norms, 0)
    for u in range(5):
        landed(u)

    def written(m, f=0):
        copies = []
        for block in range(NZ):
            if m < 2:
                source, at, n = (og, ou)[m].at[block], block * 2 * LANES, 2 * LANES
            else:
                source, at, n = od.at[f, block], (block * 2 + f) * LANES, LANES
            out = (g_out, u_out, d_out)[m].at[:, pl.ds(at, n)]
            copies.append(pltpu.make_async_copy(source, out, osem.at[(m + f) * NZ + block]))
        return copies

    for m in range(2):
        for copy in written(m):
            copy.start()

    tile = slots // 4

    def hide(i, carry):
        at = pl.ds(pl.multiple_of(i * tile, 16), tile)
        gate = jnp.zeros((tile, width), jnp.float32)
        up = jnp.zeros((tile, width), jnp.float32)
        for block in range(NZ):
            v = xall[block, at, :]
            gate = gate + lax.dot_general(v, og[block], ROWS, preferred_element_type=jnp.float32)
            up = up + lax.dot_general(v, ou[block], ROWS, preferred_element_type=jnp.float32)
        inverse = inv_ref[at, :]
        gate = gate * inverse
        up = up * inverse
        hidden[at, :] = (gate / (1.0 + jnp.exp(-gate)) * up).astype(jnp.bfloat16)
        return carry

    lax.fori_loop(0, slots // tile, hide, 0)
    second(6)

    def block_at(k):
        return lax.rem(z + (2 * lax.rem(k, 2) - 1) * ((k + 1) // 2) + NZ, NZ)

    def half_rows(which):
        return pl.ds(pl.multiple_of(which * half_slots, 16), half_slots)

    def quarter_rows(which, q):
        return pl.ds(pl.multiple_of(which * half_slots + q * quarter, 16), quarter)

    full = (theirs, got, mine, joint, far)
    thin = (theirs_h, got_h, mine_h, joint_h, far_h)

    def lanes(f):
        return pl.ds(0, 2 * LANES) if f is None else pl.ds(f * LANES, LANES)

    def spot(k, f):
        if f is None:
            return full, k, k
        at = k - FULL + f * (NZ - FULL)
        return thin, at, at + FULL

    def pair_copy(k, f):
        bufs, at, sem = spot(k, f)
        return pltpu.make_async_remote_copy(
            src_ref=bufs[0].at[at],
            dst_ref=bufs[1].at[at],
            send_sem=psend.at[sem],
            recv_sem=precv.at[sem],
            device_id=partner,
            device_id_type=MESH,
        )

    def home_copy(k, f):
        bufs, at, sem = spot(k, f)
        return pltpu.make_async_remote_copy(
            src_ref=bufs[3].at[at],
            dst_ref=parts.at[0, half_rows(core), lanes(f)],
            send_sem=fsend.at[sem * 2],
            recv_sem=rrecv.at[8],
            device_id=partner,
            device_id_type=MESH,
        )

    def far_copy(k, f, q):
        bufs, at, sem = spot(k, f)
        return pltpu.make_async_remote_copy(
            src_ref=bufs[3].at[at, pl.ds(q * quarter, quarter), :],
            dst_ref=bufs[4].at[at],
            send_sem=fsend.at[sem * 2 + q],
            recv_sem=frecv.at[sem * 2 + q],
            device_id=mate(1 - 2 * q),
            device_id_type=MESH,
        )

    def near_copy(k, f, q, side):
        bufs, at, sem = spot(k, f)
        return pltpu.make_async_remote_copy(
            src_ref=bufs[3].at[at, pl.ds(q * quarter, quarter), :],
            dst_ref=parts.at[1 + side, quarter_rows(core, q), lanes(f)],
            send_sem=fsend.at[sem * 2 + q],
            recv_sem=rrecv.at[side * 4 + core * 2 + q],
            device_id={"tp": block_at(k)},
            device_id_type=MESH,
        )

    def role(k):
        to = block_at(k)
        return to, lax.rem(to // 2 - x + NX, NX)

    def project(k, f):
        bufs, at, _ = spot(k, f)
        block = block_at(k)
        if f is None:
            weights = jnp.concatenate([od[0, block], od[1, block]], axis=1)
        else:
            weights = od[f, block]
        bufs[0][at] = lax.dot_general(
            hidden[half_rows(1 - core), :], weights, COLS, preferred_element_type=jnp.float32
        ).astype(jnp.bfloat16)
        pair_copy(k, f).start()
        bufs[2][at] = lax.dot_general(
            hidden[half_rows(core), :], weights, COLS, preferred_element_type=jnp.float32
        ).astype(jnp.bfloat16)

    def join(k, f):
        bufs, at, _ = spot(k, f)
        to, which = role(k)
        pair_copy(k, f).wait_recv()
        bufs[3][at] = (
            bufs[2][at].astype(jnp.float32) + bufs[1][at].astype(jnp.float32)
        ).astype(jnp.bfloat16)

        @pl.when(to == tp)
        def _():
            parts[0, half_rows(core), lanes(f)] = bufs[3][at]

        @pl.when((which == 0) & (to != tp))
        def _():
            home_copy(k, f).start()

        @pl.when(which == 2)
        def _():
            far_copy(k, f, 0).start()
            far_copy(k, f, 1).start()

        @pl.when(which == 1)
        def _():
            near_copy(k, f, 1, 0).start()

        @pl.when(which == 3)
        def _():
            near_copy(k, f, 0, 1).start()

    def pass_on(k, f):
        bufs, at, _ = spot(k, f)
        _, which = role(k)
        for when, q, side in ((1, 0, 0), (3, 1, 1)):

            @pl.when(which == when)
            def _():
                far_copy(k, f, q).wait_recv()
                piece = pl.ds(q * quarter, quarter)
                bufs[3][at, piece, :] = (
                    bufs[3][at, piece, :].astype(jnp.float32) + bufs[4][at].astype(jnp.float32)
                ).astype(jnp.bfloat16)
                near_copy(k, f, q, side).start()

    def sent(k, f):
        to, which = role(k)
        pair_copy(k, f).wait_send()

        @pl.when((which == 0) & (to != tp))
        def _():
            home_copy(k, f).wait_send()

        @pl.when(which != 0)
        def _():
            far_copy(k, f, 0).wait_send()
            far_copy(k, f, 1).wait_send()

    def over(what, f):
        lo, hi = (0, FULL) if f is None else (FULL, NZ)

        def step(k, carry):
            what(k, f)
            return carry

        lax.fori_loop(lo, hi, step, 0)

    over(project, None)
    over(join, None)
    landed(5)
    over(project, 0)
    over(join, 0)
    over(pass_on, None)
    landed(6)
    over(project, 1)
    for f in range(2):
        for copy in written(2, f):
            copy.start()
    over(join, 1)
    over(pass_on, 0)
    over(pass_on, 1)

    def whole_wait(place, sem):
        pltpu.make_async_remote_copy(
            src_ref=place,
            dst_ref=place,
            send_sem=fsend.at[0],
            recv_sem=rrecv.at[sem],
            device_id=partner,
            device_id_type=MESH,
        ).wait_recv()

    whole_wait(parts.at[0, half_rows(1 - core), :], 8)
    for side in range(2):
        for c in range(2):
            for q in range(2):
                whole_wait(parts.at[1 + side, quarter_rows(c, q), :], side * 4 + c * 2 + q)

    def total(at):
        value = parts[0, at, :].astype(jnp.float32)
        for block in range(1, 3):
            value = value + parts[block, at, :].astype(jnp.float32)
        ret[at, :] = value.astype(jnp.bfloat16)

    for dz, dy in group:
        total(arrived_rows(dz, yat(dy)))
        back_copy(dz, dy).start()
    total(arrived_rows(0, y))
    back[here] = ret[arrived_rows(0, y), :]
    for dz, dy in group:
        back_copy(dz, dy, True).wait_recv()

    count = tok_ref.shape[0]
    piece = count // 3

    def mix(i, carry):
        ids = lax.broadcasted_iota(jnp.int32, (piece, slots), 1)
        on = lax.broadcasted_iota(jnp.int32, (piece, count), 1) == (
            lax.broadcasted_iota(jnp.int32, (piece, count), 0) + i * piece
        )

        def column(line):
            return jnp.sum(jnp.where(on, line, 0.0), axis=1, keepdims=True)

        results = back[...].reshape(slots, back.shape[2])
        scores = [column(logit_ref[k : k + 1, :]) for k in range(2)]
        value = jnp.zeros((piece, back.shape[2]), jnp.float32)
        for k in range(2):
            wanted = column(slot_ref[k : k + 1, :].astype(jnp.float32)).astype(jnp.int32)
            chosen = jnp.where(ids == wanted, 1.0, 0.0).astype(jnp.bfloat16)
            picked = jnp.dot(chosen, results, preferred_element_type=jnp.float32)
            value = value + picked * jax.nn.sigmoid(scores[k] - scores[1 - k])
        mix_ref[pl.ds(pl.multiple_of(i * piece, 16), piece), :] = value.astype(jnp.bfloat16)
        return carry

    lax.fori_loop(0, count // piece, mix, 0)

    for u in range(UNITS):
        for dy in (1, 3, 2):
            ycopy(u, dy, y).wait_send()
        for kind in "abcd":
            for sign in (1, -1):
                zcopy(u, kind, sign).wait_send()
    for dz, dy in group:
        tokens_copy(dz, dy).wait_send()
        back_copy(dz, dy).wait_send()
    for step in range(1, NX):
        gather_copy(step).wait_send()
    for step in range(NX):
        relay_copy(step).wait_send()
    for f in (None, 0, 1):
        over(sent, f)
    for m, f in ((0, 0), (1, 0), (2, 0), (2, 1)):
        for copy in written(m, f):
            copy.wait()


def whole(gate, up, down, gain, tokens, routes, logits):
    _, rows, width = gate.shape
    count, features = tokens.shape
    most = count // 2
    split = [w.reshape(2, NY, rows, width) for w in (gate, up, down)]
    bf16 = jnp.bfloat16
    out = jax.ShapeDtypeStruct((width, NZ * 2 * LANES), bf16)
    dma = lambda n: pltpu.SemaphoreType.DMA((n,))
    vmem = lambda *shape, dtype=bf16: pltpu.VMEM(shape, dtype)
    total = EXPERTS * most
    late = 2 * (NZ - FULL)
    steps = FULL + late
    sums = [vmem(FULL, total // 2, features)] * 4 + [vmem(FULL, total // 4, features)]
    sums += [vmem(late, total // 2, LANES)] * 4 + [vmem(late, total // 4, LANES)]
    return pl.pallas_call(
        whole_kernel,
        out_shape=(out, out, out, jax.ShapeDtypeStruct((count, features), bf16)),
        in_specs=[pl.BlockSpec(memory_space=pltpu.HBM)] * 7,
        out_specs=(pl.BlockSpec(memory_space=pl.ANY),) * 3
        + (pl.BlockSpec(memory_space=pltpu.VMEM),),
        scratch_shapes=[
            vmem(NZ, width, 2 * LANES),
            vmem(NZ, width, 2 * LANES),
            vmem(2, NZ, width, LANES),
            *[pltpu.VMEM(a.shape, a.dtype) for a in (*split, gain, tokens, routes, logits)],
            vmem(2, 2, NY, rows, width),
            vmem(3, 2, NY * rows, width),
            vmem(2, width, 2 * LANES),
            vmem(2, width, LANES),
            vmem(8, count, dtype=jnp.int32),
            vmem(EXPERTS, most, features),
            vmem(2 * NX, total, features),
            vmem(total, 1, dtype=jnp.float32),
            vmem(total, width),
            *sums,
            vmem(3, total, features),
            vmem(total, features),
            vmem(EXPERTS, most, features),
            dma(3 * UNITS), dma(3 * UNITS), dma(8 * UNITS), dma(8 * UNITS),
            dma(3 * NY), dma(3 * NY), dma(2 * NX), dma(2 * NX),
            dma(steps), dma(steps), dma(2 * steps), dma(2 * steps), dma(9), dma(3 * NY), dma(3 * NY), dma(7), dma(4 * NZ),
        ],
        compiler_params=pltpu.CompilerParams(
            collective_id=0, has_side_effects=True, vmem_limit_bytes=VMEM_LIMIT
        ),
        cost_estimate=pl.CostEstimate(flops=10**11, bytes_accessed=10**7, transcendentals=0),
    )(*split, gain, tokens, routes, logits)


def shards(tokens, norm_gain, gate_train, up_train, down_train, routes, route_logits):
    *turned, mixed = whole(
        gate_train, up_train, down_train, norm_gain[None, :], tokens, routes.T, route_logits.T
    )
    return (*[w.T[None] for w in turned], mixed)


def solution(mesh):
    placed = (
        P("fs", "tp"),
        P("fs"),
        P(None, "fs", "tp"),
        P(None, "fs", "tp"),
        P(None, "fs", "tp"),
        P("fs", None),
        P("fs", None),
    )
    return jax.shard_map(
        shards,
        mesh=mesh,
        in_specs=placed,
        out_specs=(P("fs", None, "tp"), P("fs", None, "tp"), P("fs", None, "tp"), P("fs", "tp")),
        check_vma=False,
    )
```

```python
import functools

import jax
import jax.numpy as jnp
from jax import lax
from jax.experimental import pallas as pl
from jax.experimental.pallas import tpu as pltpu
from jax.sharding import PartitionSpec as P

EXPERTS = 8
epsilon = 1e-06
MESH = pl.DeviceIdType.MESH
NZ, NY = 8, 4
VMEM_LIMIT = 40 * 1024 * 1024
NZ, NY, NX = 8, 4, 4
LANES = 128
SPLIT = ((0, 0, 128), (0, 128, 256), (0, 384, 320), (1, 0, 384), (1, 384, 320))
DOWN = ((2, 0, 384), (2, 384, 320))
ACROSS = SPLIT + DOWN
UNITS = len(SPLIT) + 2
COLS = (((1,), (0,)), ((), ()))
ROWS = (((1,), (1,)), ((), ()))
NEAR = 5


def whole_kernel(
    g_in, u_in, d_in, gain_in, tok_in, route_in, logit_in,
    og, ou, od, mix_ref,
    g_ref, u_ref, d_ref, gain_ref, tok_ref, route_ref, logit_ref, scaled, ybuf, away, awayd, slot_ref, xs, xall, inv_ref, hidden,
    theirs, got, mine, joint, far, parts, ret, back,
    ysend, yrecv, zsend, zrecv, tsend, trecv, asend, arecv, psend, precv, fsend, frecv, rrecv, bsend, brecv, lsem,
):
    fs = lax.axis_index("fs")
    tp = lax.axis_index("tp")
    z, y = fs // NY, lax.rem(fs, NY)
    x, core = tp // 2, lax.rem(tp, 2)
    parity = lax.rem(z, 2)
    sources = (scaled.at[0], scaled.at[1], d_ref)
    rows = g_ref.shape[2]
    width = g_ref.shape[3]
    most = xs.shape[1]
    few = most // 2
    slots = xall.shape[1]
    half_slots = slots // 2
    quarter = slots // 4
    here = parity * NY + y

    def zat(step):
        return lax.rem(z + step + NZ, NZ)

    def yat(step):
        return lax.rem(y + step + NY, NY)

    def device(dz, dy):
        return {"fs": zat(dz) * NY + yat(dy)}

    def mate(step):
        return {"tp": lax.rem(x + step + NX, NX) * 2 + core}

    partner = {"tp": x * 2 + 1 - core}
    group = [(dz, dy) for dz, dys in ((1, (0, 1, 3, 2)), (-1, (0, 1, 3, 2)), (0, (1, 3, 2))) for dy in dys]

    loads = [
        pltpu.make_async_copy(source, held, lsem.at[i])
        for i, (source, held) in enumerate(
            (
                (g_in, g_ref),
                (gain_in, gain_ref),
                (route_in, route_ref),
                (tok_in, tok_ref),
                (u_in, u_ref),
                (d_in, d_ref),
                (logit_in, logit_ref),
            )
        )
    ]
    for load in loads:
        load.start()
    barrier = pltpu.get_barrier_semaphore()
    greeted = [device(dz, dy) for dz, dy in group + [(2, 0), (-2, 0)]]
    greeted += [{"tp": lax.rem(tp + step, 2 * NX)} for step in range(1, 2 * NX)]
    for other in greeted:
        pl.semaphore_signal(barrier, inc=1, device_id=other, device_id_type=MESH)
    pl.semaphore_wait(barrier, len(greeted))

    def ycopy(u, dy, to_row):
        m, lo, n = ACROSS[u]
        return pltpu.make_async_remote_copy(
            src_ref=sources[m].at[:, yat(dy), :, pl.ds(lo, n)],
            dst_ref=ybuf.at[m, :, pl.ds(to_row * rows, rows), pl.ds(lo, n)],
            send_sem=ysend.at[u * 3 + dy - 1],
            recv_sem=yrecv.at[u * 3 + dy - 1],
            device_id=device(0, dy),
            device_id_type=MESH,
        )

    def zcopy(u, kind, sign, arriving=False):
        if u < len(SPLIT):
            m, lo, n = SPLIT[u]
            out, left = (og, ou)[m], away.at[m]
        else:
            lo, n = 0, width
            out, left = od.at[u - len(SPLIT)], awayd.at[u - len(SPLIT)]
        near = {"a": 1, "b": 2, "c": 2, "d": 2}[kind]
        hops = {"a": 0, "b": 0, "c": 1, "d": 2}[kind]
        block = zat(-sign * hops)
        if arriving:
            block = zat(-sign * (hops + near))
        if kind == "d":
            half = n // 2
            lo, n = (lo, half) if sign > 0 else (lo + half, half)
        place = out.at[block, pl.ds(lo, n), :]
        source = left.at[pl.ds(lo, n), :] if kind == "a" else place
        at = u * 8 + "abcd".index(kind) * 2 + (0 if sign > 0 else 1)
        return pltpu.make_async_remote_copy(
            src_ref=source,
            dst_ref=place,
            send_sem=zsend.at[at],
            recv_sem=zrecv.at[at],
            device_id=device(sign * near, 0),
            device_id_type=MESH,
        )

    def base(dz):
        return {0: 0, 1: half_slots, -1: half_slots + quarter}[dz]

    def arrived_rows(dz, at_y):
        n = few if dz else most
        return pl.ds(pl.multiple_of(base(dz) + at_y * n, 16), n)

    def held_rows(dz):
        return pl.ds({0: 0, 1: 0, -1: few}[dz], few if dz else most)

    def expert(dz, at_y):
        return ((1 - parity) if dz else parity) * NY + at_y

    def tokens_copy(dz, dy, arriving=False):
        at = (dz + 1) * NY + dy
        return pltpu.make_async_remote_copy(
            src_ref=xs.at[expert(dz, yat(dy)), held_rows(dz), :],
            dst_ref=xall.at[tp, arrived_rows(dz, yat(-dy) if arriving else y), :],
            send_sem=tsend.at[at],
            recv_sem=trecv.at[at],
            device_id=device(dz, dy),
            device_id_type=MESH,
        )

    def back_copy(dz, dy, arriving=False):
        at = (dz + 1) * NY + dy
        owner = expert(dz, yat(-dy)) if arriving else here
        return pltpu.make_async_remote_copy(
            src_ref=ret.at[arrived_rows(dz, yat(dy)), :],
            dst_ref=back.at[owner, held_rows(dz), :],
            send_sem=bsend.at[at],
            recv_sem=brecv.at[at],
            device_id=device(-dz, dy),
            device_id_type=MESH,
        )

    def gather_copy(step, arriving=False):
        block = lax.rem(x - step + NX, NX) * 2 + core if arriving else tp
        return pltpu.make_async_remote_copy(
            src_ref=xall.at[tp],
            dst_ref=xall.at[block],
            send_sem=asend.at[step],
            recv_sem=arecv.at[step],
            device_id=mate(step),
            device_id_type=MESH,
        )

    def relay_copy(step, arriving=False):
        block = lax.rem(x - step + NX, NX) * 2 + core
        if arriving:
            block = lax.rem(x - step + NX, NX) * 2 + 1 - core
        return pltpu.make_async_remote_copy(
            src_ref=xall.at[block],
            dst_ref=xall.at[block],
            send_sem=asend.at[NX + step],
            recv_sem=arecv.at[NX + step],
            device_id=partner,
            device_id_type=MESH,
        )

    def scale(m, ref):
        wide = gain_ref[...]
        on = lax.broadcasted_iota(jnp.int32, (rows, rows), 0) == lax.broadcasted_iota(
            jnp.int32, (rows, rows), 1
        )
        gain = jnp.sum(jnp.where(on, wide, 0.0), axis=1, keepdims=True)

        def one(e, carry):
            block = ref[e // NY, lax.rem(e, NY)]
            scaled[m, e // NY, lax.rem(e, NY)] = (block.astype(jnp.float32) * gain).astype(
                jnp.bfloat16
            )
            return carry

        lax.fori_loop(0, EXPERTS, one, 0)

    def across(m):
        for u, (owner, lo, n) in enumerate(ACROSS):
            if owner == m:
                for dy in (1, 3, 2):
                    ycopy(u, dy, y).start()
        ybuf[m, :, pl.ds(y * rows, rows), :] = sources[m][:, y]

    def plan():
        count = tok_ref.shape[0]
        lines = lax.broadcasted_iota(jnp.int32, (2 * EXPERTS, count), 0)
        routes = route_ref[...]
        named = (routes[0:1, :] == lines) | (routes[1:2, :] == lines - EXPERTS)
        named = jnp.where(named, 1.0, 0.0)
        before = jnp.where(
            lax.broadcasted_iota(jnp.int32, (count, count), 0)
            < lax.broadcasted_iota(jnp.int32, (count, count), 1),
            1.0,
            0.0,
        )
        rank = jnp.dot(
            named.astype(jnp.bfloat16),
            before.astype(jnp.bfloat16),
            preferred_element_type=jnp.float32,
        )
        for k in range(2):
            one = named[k * EXPERTS : (k + 1) * EXPERTS]
            place = rank[k * EXPERTS : (k + 1) * EXPERTS]
            if k:
                place = place + jnp.sum(named[:EXPERTS], axis=1, keepdims=True)
            place = place + (lines[:EXPERTS] * most).astype(jnp.float32)
            slot = jnp.sum(one * place, axis=0, keepdims=True)
            slot_ref[k : k + 1, :] = slot.astype(jnp.int32)

    for load in loads[:2]:
        load.wait()
    scale(0, g_ref)
    across(0)
    for load in loads[2:]:
        load.wait()
    plan()

    def pick(e, carry):
        ids = lax.broadcasted_iota(jnp.int32, (most, tok_ref.shape[0]), 0) + e * most
        hit = (ids == slot_ref[0:1, :]) | (ids == slot_ref[1:2, :])
        chosen = jnp.where(hit, 1.0, 0.0).astype(jnp.bfloat16)
        xs[e] = jnp.dot(chosen, tok_ref[...], preferred_element_type=jnp.float32).astype(
            jnp.bfloat16
        )
        return carry

    lax.fori_loop(0, EXPERTS, pick, 0)
    for dz, dy in group:
        tokens_copy(dz, dy).start()
    xall[tp, arrived_rows(0, y), :] = xs[here]
    scale(1, u_ref)
    across(1)
    across(2)

    def turn(u):
        if u < len(SPLIT):
            m, lo, n = SPLIT[u]
            for dy in (1, 3, 2):
                ycopy(u, dy, yat(-dy)).wait_recv()
            away[m, pl.ds(lo, n), :] = ybuf[m, 1 - parity, :, lo : lo + n].T
            (og, ou)[m][z, pl.ds(lo, n), :] = ybuf[m, parity, :, lo : lo + n].T
        elif u == len(SPLIT):
            for part, (m, lo, n) in enumerate(DOWN):
                for dy in (1, 3, 2):
                    ycopy(u + part, dy, yat(-dy)).wait_recv()
                gone = ybuf[m, 1 - parity, :, lo : lo + n].T
                kept = ybuf[m, parity, :, lo : lo + n].T
                for f in range(2):
                    awayd[f, pl.ds(lo, n), :] = gone[:, f * LANES : (f + 1) * LANES]
                    od[f, z, pl.ds(lo, n), :] = kept[:, f * LANES : (f + 1) * LANES]

    def first(u):
        turn(u)
        for kind in "ba" if u >= len(SPLIT) else "ab":
            for sign in (1, -1):
                zcopy(u, kind, sign).start()

    def second(u, kinds="ab"):
        for kind in kinds:
            for sign in (1, -1):
                zcopy(u, kind, sign, True).wait_recv()
                zcopy(u, {"a": "c", "b": "d"}[kind], sign).start()

    def landed(u, kinds="cd"):
        for kind in kinds:
            for sign in (1, -1):
                zcopy(u, kind, sign, True).wait_recv()

    first(0)
    first(1)
    second(0)
    first(2)
    for dz, dy in group:
        tokens_copy(dz, dy, True).wait_recv()
    for step in (1, 3, 2):
        gather_copy(step).start()
    relay_copy(0).start()
    second(1)
    first(3)
    second(2)
    first(4)
    for step in (1, 3):
        gather_copy(step, True).wait_recv()
        relay_copy(step).start()
    second(3)
    gather_copy(2, True).wait_recv()
    relay_copy(2).start()
    second(4)
    first(5)
    first(6)
    for step in range(NX):
        relay_copy(step, True).wait_recv()

    def norms(i, carry):
        at = pl.ds(pl.multiple_of(i * most, 16), most)
        total = jnp.zeros((most, 1), jnp.float32)
        for block in range(xall.shape[0]):
            v = xall[block, at, :].astype(jnp.float32)
            total = total + jnp.sum(v * v, axis=1, keepdims=True)
        mean = total / (xall.shape[0] * xall.shape[2])
        inv_ref[at, :] = lax.rsqrt(mean + epsilon)
        return carry

    lax.fori_loop(0, EXPERTS, norms, 0)
    for u in range(5):
        landed(u)

    tile = slots // 4

    def hide(i, carry):
        at = pl.ds(pl.multiple_of(i * tile, 16), tile)
        gate = jnp.zeros((tile, width), jnp.float32)
        up = jnp.zeros((tile, width), jnp.float32)
        for block in range(NZ):
            v = xall[block, at, :]
            gate = gate + lax.dot_general(v, og[block], ROWS, preferred_element_type=jnp.float32)
            up = up + lax.dot_general(v, ou[block], ROWS, preferred_element_type=jnp.float32)
        inverse = inv_ref[at, :]
        gate = gate * inverse
        up = up * inverse
        hidden[at, :] = (gate / (1.0 + jnp.exp(-gate)) * up).astype(jnp.bfloat16)
        return carry

    lax.fori_loop(0, slots // tile, hide, 0)
    second(5, "b")
    for sign in (1, -1):
        zcopy(5, "a", sign, True).wait_recv()

    def block_at(k):
        return lax.rem(z + (2 * lax.rem(k, 2) - 1) * ((k + 1) // 2) + NZ, NZ)

    def half_rows(which):
        return pl.ds(pl.multiple_of(which * half_slots, 16), half_slots)

    def quarter_rows(which, q):
        return pl.ds(pl.multiple_of(which * half_slots + q * quarter, 16), quarter)

    bufs = (theirs, got, mine, joint, far)

    def lanes(f):
        return pl.ds(f * LANES, LANES)

    def pair_copy(k, f):
        at = f * NZ + k
        return pltpu.make_async_remote_copy(
            src_ref=bufs[0].at[at],
            dst_ref=bufs[1].at[at],
            send_sem=psend.at[at],
            recv_sem=precv.at[at],
            device_id=partner,
            device_id_type=MESH,
        )

    def home_copy(k, f):
        at = f * NZ + k
        return pltpu.make_async_remote_copy(
            src_ref=bufs[3].at[at],
            dst_ref=parts.at[0, half_rows(core), lanes(f)],
            send_sem=fsend.at[at * 2],
            recv_sem=rrecv.at[8],
            device_id=partner,
            device_id_type=MESH,
        )

    def far_copy(k, f, q):
        at = f * NZ + k
        return pltpu.make_async_remote_copy(
            src_ref=bufs[3].at[at, pl.ds(q * quarter, quarter), :],
            dst_ref=bufs[4].at[at],
            send_sem=fsend.at[at * 2 + q],
            recv_sem=frecv.at[at * 2 + q],
            device_id=mate(1 - 2 * q),
            device_id_type=MESH,
        )

    def near_copy(k, f, q, side):
        at = f * NZ + k
        return pltpu.make_async_remote_copy(
            src_ref=bufs[3].at[at, pl.ds(q * quarter, quarter), :],
            dst_ref=parts.at[1 + side, quarter_rows(core, q), lanes(f)],
            send_sem=fsend.at[at * 2 + q],
            recv_sem=rrecv.at[side * 4 + core * 2 + q],
            device_id={"tp": block_at(k)},
            device_id_type=MESH,
        )

    def role(k):
        to = block_at(k)
        return to, lax.rem(to // 2 - x + NX, NX)

    def project(k, f):
        at = f * NZ + k
        weights = od[f, block_at(k)]
        bufs[0][at] = lax.dot_general(
            hidden[half_rows(1 - core), :], weights, COLS, preferred_element_type=jnp.float32
        ).astype(jnp.bfloat16)
        pair_copy(k, f).start()
        bufs[2][at] = lax.dot_general(
            hidden[half_rows(core), :], weights, COLS, preferred_element_type=jnp.float32
        ).astype(jnp.bfloat16)

    def project_two(k, f):
        at = f * NZ + k
        weights = jnp.concatenate([od[f, block_at(k)], od[f, block_at(k + 1)]], axis=1)
        for buf, which in ((0, 1 - core), (2, core)):
            value = lax.dot_general(
                hidden[half_rows(which), :], weights, COLS, preferred_element_type=jnp.float32
            ).astype(jnp.bfloat16)
            bufs[buf][at] = value[:, :LANES]
            bufs[buf][at + 1] = value[:, LANES:]
            if buf == 0:
                pair_copy(k, f).start()
                pair_copy(k + 1, f).start()

    def project_both(k):
        block = block_at(k)
        weights = jnp.concatenate([od[0, block], od[1, block]], axis=1)
        for buf, which in ((0, 1 - core), (2, core)):
            value = lax.dot_general(
                hidden[half_rows(which), :], weights, COLS, preferred_element_type=jnp.float32
            ).astype(jnp.bfloat16)
            for f in range(2):
                bufs[buf][f * NZ + k] = value[:, f * LANES : (f + 1) * LANES]
                if buf == 0:
                    pair_copy(k, f).start()

    def join(k, f):
        at = f * NZ + k
        to, which = role(k)
        pair_copy(k, f).wait_recv()
        bufs[3][at] = (
            bufs[2][at].astype(jnp.float32) + bufs[1][at].astype(jnp.float32)
        ).astype(jnp.bfloat16)

        @pl.when(to == tp)
        def _():
            parts[0, half_rows(core), lanes(f)] = bufs[3][at]

        @pl.when((which == 0) & (to != tp))
        def _():
            home_copy(k, f).start()

        @pl.when(which == 2)
        def _():
            far_copy(k, f, 0).start()
            far_copy(k, f, 1).start()

        @pl.when(which == 1)
        def _():
            near_copy(k, f, 1, 0).start()

        @pl.when(which == 3)
        def _():
            near_copy(k, f, 0, 1).start()

    def pass_on(k, f):
        at = f * NZ + k
        _, which = role(k)
        for when, q, side in ((1, 0, 0), (3, 1, 1)):

            @pl.when(which == when)
            def _():
                far_copy(k, f, q).wait_recv()
                piece = pl.ds(q * quarter, quarter)
                bufs[3][at, piece, :] = (
                    bufs[3][at, piece, :].astype(jnp.float32) + bufs[4][at].astype(jnp.float32)
                ).astype(jnp.bfloat16)
                near_copy(k, f, q, side).start()

    def sent(k, f):
        to, which = role(k)
        pair_copy(k, f).wait_send()

        @pl.when((which == 0) & (to != tp))
        def _():
            home_copy(k, f).wait_send()

        @pl.when(which != 0)
        def _():
            far_copy(k, f, 0).wait_send()
            far_copy(k, f, 1).wait_send()

    def near(f):
        project_two(0, f)
        project_two(2, f)
        join(0, f)
        join(1, f)
        project(4, f)
        for k in (2, 3, 4):
            join(k, f)

    def whole_wait(place, sem):
        pltpu.make_async_remote_copy(
            src_ref=place,
            dst_ref=place,
            send_sem=fsend.at[0],
            recv_sem=rrecv.at[sem],
            device_id=partner,
            device_id_type=MESH,
        ).wait_recv()

    def total(c, q):
        at = quarter_rows(c, q)
        value = parts[0, at, :].astype(jnp.float32)
        for side in range(2):
            whole_wait(parts.at[1 + side, at, :], side * 4 + c * 2 + q)
            value = value + parts[1 + side, at, :].astype(jnp.float32)
        ret[at, :] = value.astype(jnp.bfloat16)

    def give_back():
        whole_wait(parts.at[0, half_rows(1 - core), :], 8)
        for q, dz in ((0, 1), (1, -1)):
            total(1, q)
            for dy in (0, 1, 3, 2):
                back_copy(dz, dy).start()
        total(0, 0)
        total(0, 1)
        for dy in (1, 3, 2):
            back_copy(0, dy).start()
        back[here] = ret[arrived_rows(0, y), :]

    away_by = lax.rem(tp - z + NZ, NZ)
    early = (away_by <= 2) | (away_by >= 6)

    near(0)
    second(6, "b")
    for sign in (1, -1):
        zcopy(5, "c", sign).start()
    second(6, "a")
    near(1)
    for k in range(NEAR):
        pass_on(k, 0)
    landed(5, "d")
    landed(6, "d")
    project_both(NZ - 1)
    for f in range(2):
        join(NZ - 1, f)
    for k in range(NEAR):
        pass_on(k, 1)
    landed(5, "c")
    project_two(NEAR, 0)
    for f in range(2):
        pass_on(NZ - 1, f)
    for k in (NEAR, NEAR + 1):
        join(k, 0)

    @pl.when(early)
    def _():
        give_back()

    landed(6, "c")
    project_two(NEAR, 1)
    for k in (NEAR, NEAR + 1):
        join(k, 1)
    for f in range(2):
        for k in (NEAR, NEAR + 1):
            pass_on(k, f)

    @pl.when(jnp.logical_not(early))
    def _():
        give_back()

    for dz, dy in group:
        back_copy(dz, dy, True).wait_recv()

    count = tok_ref.shape[0]
    piece = count // 3

    def mix(i, carry):
        ids = lax.broadcasted_iota(jnp.int32, (piece, slots), 1)
        on = lax.broadcasted_iota(jnp.int32, (piece, count), 1) == (
            lax.broadcasted_iota(jnp.int32, (piece, count), 0) + i * piece
        )

        def column(line):
            return jnp.sum(jnp.where(on, line, 0.0), axis=1, keepdims=True)

        results = back[...].reshape(slots, back.shape[2])
        scores = [column(logit_ref[k : k + 1, :]) for k in range(2)]
        value = jnp.zeros((piece, back.shape[2]), jnp.float32)
        for k in range(2):
            wanted = column(slot_ref[k : k + 1, :].astype(jnp.float32)).astype(jnp.int32)
            chosen = jnp.where(ids == wanted, 1.0, 0.0).astype(jnp.bfloat16)
            picked = jnp.dot(chosen, results, preferred_element_type=jnp.float32)
            value = value + picked * jax.nn.sigmoid(scores[k] - scores[1 - k])
        mix_ref[pl.ds(pl.multiple_of(i * piece, 16), piece), :] = value.astype(jnp.bfloat16)
        return carry

    lax.fori_loop(0, count // piece, mix, 0)

    for u in range(UNITS):
        for dy in (1, 3, 2):
            ycopy(u, dy, y).wait_send()
        for kind in "abcd":
            for sign in (1, -1):
                zcopy(u, kind, sign).wait_send()
    for dz, dy in group:
        tokens_copy(dz, dy).wait_send()
        back_copy(dz, dy).wait_send()
    for step in range(1, NX):
        gather_copy(step).wait_send()
    for step in range(NX):
        relay_copy(step).wait_send()
    for f in range(2):
        lax.fori_loop(0, NZ, lambda k, carry: (sent(k, f), carry)[1], 0)


def whole(gate, up, down, gain, tokens, routes, logits):
    _, rows, width = gate.shape
    count, features = tokens.shape
    most = count // 2
    split = [w.reshape(2, NY, rows, width) for w in (gate, up, down)]
    given = (*split, gain, tokens, routes, logits)
    bf16 = jnp.bfloat16
    out = jax.ShapeDtypeStruct((NZ, width, 2 * LANES), bf16)
    dma = lambda n: pltpu.SemaphoreType.DMA((n,))
    vmem = lambda *shape, dtype=bf16: pltpu.VMEM(shape, dtype)
    total = EXPERTS * most
    steps = 2 * NZ
    sums = [vmem(steps, total // 2, LANES)] * 4 + [vmem(steps, total // 4, LANES)]
    return pl.pallas_call(
        whole_kernel,
        out_shape=(
            out,
            out,
            jax.ShapeDtypeStruct((2, NZ, width, LANES), bf16),
            jax.ShapeDtypeStruct((count, features), bf16),
        ),
        in_specs=[pl.BlockSpec(memory_space=pltpu.HBM)] * 7,
        out_specs=(pl.BlockSpec(memory_space=pltpu.VMEM),) * 4,
        scratch_shapes=[
            *[pltpu.VMEM(a.shape, a.dtype) for a in given],
            vmem(2, 2, NY, rows, width),
            vmem(3, 2, NY * rows, width),
            vmem(2, width, 2 * LANES),
            vmem(2, width, LANES),
            vmem(8, count, dtype=jnp.int32),
            vmem(EXPERTS, most, features),
            vmem(2 * NX, total, features),
            vmem(total, 1, dtype=jnp.float32),
            vmem(total, width),
            *sums,
            vmem(3, total, features),
            vmem(total, features),
            vmem(EXPERTS, most, features),
            dma(3 * UNITS), dma(3 * UNITS), dma(8 * UNITS), dma(8 * UNITS),
            dma(3 * NY), dma(3 * NY), dma(2 * NX), dma(2 * NX),
            dma(steps), dma(steps), dma(2 * steps), dma(2 * steps), dma(9), dma(3 * NY), dma(3 * NY), dma(7),
        ],
        compiler_params=pltpu.CompilerParams(
            collective_id=0, has_side_effects=True, vmem_limit_bytes=VMEM_LIMIT
        ),
        cost_estimate=pl.CostEstimate(flops=10**11, bytes_accessed=10**7, transcendentals=0),
    )(*[pltpu.with_memory_space_constraint(a, pltpu.HBM) for a in given])


def place_kernel(g_ref, u_ref, d_ref, m_ref, og, ou, od, om, sem):
    copies = [pltpu.make_async_copy(m_ref, om, sem.at[4 * NZ])]
    for m, (ref, out) in enumerate(((g_ref, og), (u_ref, ou))):
        for block in range(NZ):
            columns = pl.ds(block * 2 * LANES, 2 * LANES)
            copies.append(
                pltpu.make_async_copy(ref.at[block], out.at[:, columns], sem.at[m * NZ + block])
            )
    for f in range(2):
        for block in range(NZ):
            columns = pl.ds((block * 2 + f) * LANES, LANES)
            at = (2 + f) * NZ + block
            copies.append(pltpu.make_async_copy(d_ref.at[f, block], od.at[:, columns], sem.at[at]))
    for copy in copies:
        copy.start()
    for copy in copies:
        copy.wait()


def placed_out(blocks):
    nz, width, size = blocks[0].shape
    out = jax.ShapeDtypeStruct((width, nz * size), jnp.bfloat16)
    *turned, mixed = pl.pallas_call(
        place_kernel,
        out_shape=(out, out, out, jax.ShapeDtypeStruct(blocks[3].shape, jnp.bfloat16)),
        in_specs=[pl.BlockSpec(memory_space=pltpu.VMEM)] * 4,
        out_specs=(pl.BlockSpec(memory_space=pl.ANY),) * 4,
        scratch_shapes=[pltpu.SemaphoreType.DMA((4 * NZ + 1,))],
        compiler_params=pltpu.CompilerParams(vmem_limit_bytes=2 * 1024 * 1024),
    )(*blocks)
    return (*[w.T[None] for w in turned], mixed)


def shards(tokens, norm_gain, gate_train, up_train, down_train, routes, route_logits):
    return placed_out(
        whole(
            gate_train, up_train, down_train, norm_gain[None, :], tokens, routes.T, route_logits.T
        )
    )


def solution(mesh):
    placed = (
        P("fs", "tp"),
        P("fs"),
        P(None, "fs", "tp"),
        P(None, "fs", "tp"),
        P(None, "fs", "tp"),
        P("fs", None),
        P("fs", None),
    )
    return jax.shard_map(
        shards,
        mesh=mesh,
        in_specs=placed,
        out_specs=(P("fs", None, "tp"), P("fs", None, "tp"), P("fs", None, "tp"), P("fs", "tp")),
        check_vma=False,
    )
```

```python
import functools

import jax
import jax.numpy as jnp
from jax import lax
from jax.experimental import pallas as pl
from jax.experimental.pallas import tpu as pltpu
from jax.sharding import PartitionSpec as P

EXPERTS = 8
epsilon = 1e-06
MESH = pl.DeviceIdType.MESH
NZ, NY = 8, 4
VMEM_LIMIT = 40 * 1024 * 1024
NZ, NY, NX = 8, 4, 4
LANES = 128
SPLIT = ((0, 0, 128), (0, 128, 256), (0, 384, 320), (1, 0, 384), (1, 384, 320))
DOWN = ((2, 0, 384), (2, 384, 320))
ACROSS = SPLIT + DOWN
UNITS = len(SPLIT) + 2
COLS = (((1,), (0,)), ((), ()))
ROWS = (((1,), (1,)), ((), ()))
NEAR = 5


def whole_kernel(
    g_in, u_in, d_in, gain_in, tok_in, route_in, logit_in,
    og, ou, od, mix_ref,
    g_ref, u_ref, d_ref, gain_ref, tok_ref, route_ref, logit_ref, scaled, ybuf, away, awayd, slot_ref, xs, xall, inv_ref, hidden,
    theirs, got, mine, joint, far, parts, ret, back,
    ysend, yrecv, zsend, zrecv, tsend, trecv, asend, arecv, psend, precv, fsend, frecv, rrecv, bsend, brecv, lsem,
):
    fs = lax.axis_index("fs")
    tp = lax.axis_index("tp")
    z, y = fs // NY, lax.rem(fs, NY)
    x, core = tp // 2, lax.rem(tp, 2)
    parity = lax.rem(z, 2)
    sources = (scaled.at[0], scaled.at[1], d_ref)
    rows = g_ref.shape[2]
    width = g_ref.shape[3]
    most = xs.shape[1]
    few = most // 2
    slots = xall.shape[1]
    half_slots = slots // 2
    quarter = slots // 4
    here = parity * NY + y

    def zat(step):
        return lax.rem(z + step + NZ, NZ)

    def yat(step):
        return lax.rem(y + step + NY, NY)

    def device(dz, dy):
        return {"fs": zat(dz) * NY + yat(dy)}

    def mate(step):
        return {"tp": lax.rem(x + step + NX, NX) * 2 + core}

    partner = {"tp": x * 2 + 1 - core}
    group = [(dz, dy) for dz, dys in ((1, (0, 1, 3, 2)), (-1, (0, 1, 3, 2)), (0, (1, 3, 2))) for dy in dys]

    loads = [
        pltpu.make_async_copy(source, held, lsem.at[i])
        for i, (source, held) in enumerate(
            (
                (g_in, g_ref),
                (gain_in, gain_ref),
                (route_in, route_ref),
                (tok_in, tok_ref),
                (u_in, u_ref),
                (d_in, d_ref),
                (logit_in, logit_ref),
            )
        )
    ]
    for load in loads:
        load.start()
    barrier = pltpu.get_barrier_semaphore()
    greeted = [device(dz, dy) for dz, dy in group + [(2, 0), (-2, 0)]]
    greeted += [{"tp": lax.rem(tp + step, 2 * NX)} for step in range(1, 2 * NX)]
    for other in greeted:
        pl.semaphore_signal(barrier, inc=1, device_id=other, device_id_type=MESH)
    pl.semaphore_wait(barrier, len(greeted))

    def ycopy(u, dy, to_row):
        m, lo, n = ACROSS[u]
        return pltpu.make_async_remote_copy(
            src_ref=sources[m].at[:, yat(dy), :, pl.ds(lo, n)],
            dst_ref=ybuf.at[m, :, pl.ds(to_row * rows, rows), pl.ds(lo, n)],
            send_sem=ysend.at[u * 3 + dy - 1],
            recv_sem=yrecv.at[u * 3 + dy - 1],
            device_id=device(0, dy),
            device_id_type=MESH,
        )

    def zcopy(u, kind, sign, arriving=False):
        if u < len(SPLIT):
            m, lo, n = SPLIT[u]
            out, left = (og, ou)[m], away.at[m]
        else:
            lo, n = 0, width
            out, left = od.at[u - len(SPLIT)], awayd.at[u - len(SPLIT)]
        near = {"a": 1, "b": 2, "c": 2, "d": 2}[kind]
        hops = {"a": 0, "b": 0, "c": 1, "d": 2}[kind]
        block = zat(-sign * hops)
        if arriving:
            block = zat(-sign * (hops + near))
        if kind == "d":
            half = n // 2
            lo, n = (lo, half) if sign > 0 else (lo + half, half)
        place = out.at[block, pl.ds(lo, n), :]
        source = left.at[pl.ds(lo, n), :] if kind == "a" else place
        at = u * 8 + "abcd".index(kind) * 2 + (0 if sign > 0 else 1)
        return pltpu.make_async_remote_copy(
            src_ref=source,
            dst_ref=place,
            send_sem=zsend.at[at],
            recv_sem=zrecv.at[at],
            device_id=device(sign * near, 0),
            device_id_type=MESH,
        )

    def base(dz):
        return {0: 0, 1: half_slots, -1: half_slots + quarter}[dz]

    def arrived_rows(dz, at_y):
        n = few if dz else most
        return pl.ds(pl.multiple_of(base(dz) + at_y * n, 16), n)

    def held_rows(dz):
        return pl.ds({0: 0, 1: 0, -1: few}[dz], few if dz else most)

    def expert(dz, at_y):
        return ((1 - parity) if dz else parity) * NY + at_y

    def tokens_copy(dz, dy, arriving=False):
        at = (dz + 1) * NY + dy
        return pltpu.make_async_remote_copy(
            src_ref=xs.at[expert(dz, yat(dy)), held_rows(dz), :],
            dst_ref=xall.at[tp, arrived_rows(dz, yat(-dy) if arriving else y), :],
            send_sem=tsend.at[at],
            recv_sem=trecv.at[at],
            device_id=device(dz, dy),
            device_id_type=MESH,
        )

    def lanes(f):
        return pl.ds(f * LANES, LANES)

    def back_copy(dz, dy, f, arriving=False):
        at = (f * 3 + dz + 1) * NY + dy
        owner = expert(dz, yat(-dy)) if arriving else here
        return pltpu.make_async_remote_copy(
            src_ref=ret.at[arrived_rows(dz, yat(dy)), lanes(f)],
            dst_ref=back.at[owner, held_rows(dz), lanes(f)],
            send_sem=bsend.at[at],
            recv_sem=brecv.at[at],
            device_id=device(-dz, dy),
            device_id_type=MESH,
        )

    def gather_copy(step, arriving=False):
        block = lax.rem(x - step + NX, NX) * 2 + core if arriving else tp
        return pltpu.make_async_remote_copy(
            src_ref=xall.at[tp],
            dst_ref=xall.at[block],
            send_sem=asend.at[step],
            recv_sem=arecv.at[step],
            device_id=mate(step),
            device_id_type=MESH,
        )

    def relay_copy(step, arriving=False):
        block = lax.rem(x - step + NX, NX) * 2 + core
        if arriving:
            block = lax.rem(x - step + NX, NX) * 2 + 1 - core
        return pltpu.make_async_remote_copy(
            src_ref=xall.at[block],
            dst_ref=xall.at[block],
            send_sem=asend.at[NX + step],
            recv_sem=arecv.at[NX + step],
            device_id=partner,
            device_id_type=MESH,
        )

    def scale(m, ref):
        wide = gain_ref[...]
        on = lax.broadcasted_iota(jnp.int32, (rows, rows), 0) == lax.broadcasted_iota(
            jnp.int32, (rows, rows), 1
        )
        gain = jnp.sum(jnp.where(on, wide, 0.0), axis=1, keepdims=True)

        def one(e, carry):
            block = ref[e // NY, lax.rem(e, NY)]
            scaled[m, e // NY, lax.rem(e, NY)] = (block.astype(jnp.float32) * gain).astype(
                jnp.bfloat16
            )
            return carry

        lax.fori_loop(0, EXPERTS, one, 0)

    def across(m):
        for u, (owner, lo, n) in enumerate(ACROSS):
            if owner == m:
                for dy in (1, 3, 2):
                    ycopy(u, dy, y).start()
        ybuf[m, :, pl.ds(y * rows, rows), :] = sources[m][:, y]

    def plan():
        count = tok_ref.shape[0]
        lines = lax.broadcasted_iota(jnp.int32, (2 * EXPERTS, count), 0)
        routes = route_ref[...]
        named = (routes[0:1, :] == lines) | (routes[1:2, :] == lines - EXPERTS)
        named = jnp.where(named, 1.0, 0.0)
        before = jnp.where(
            lax.broadcasted_iota(jnp.int32, (count, count), 0)
            < lax.broadcasted_iota(jnp.int32, (count, count), 1),
            1.0,
            0.0,
        )
        rank = jnp.dot(
            named.astype(jnp.bfloat16),
            before.astype(jnp.bfloat16),
            preferred_element_type=jnp.float32,
        )
        for k in range(2):
            one = named[k * EXPERTS : (k + 1) * EXPERTS]
            place = rank[k * EXPERTS : (k + 1) * EXPERTS]
            if k:
                place = place + jnp.sum(named[:EXPERTS], axis=1, keepdims=True)
            place = place + (lines[:EXPERTS] * most).astype(jnp.float32)
            slot = jnp.sum(one * place, axis=0, keepdims=True)
            slot_ref[k : k + 1, :] = slot.astype(jnp.int32)

    for load in loads[:2]:
        load.wait()
    scale(0, g_ref)
    across(0)
    for load in loads[2:]:
        load.wait()
    plan()

    def pick(e, carry):
        ids = lax.broadcasted_iota(jnp.int32, (most, tok_ref.shape[0]), 0) + e * most
        hit = (ids == slot_ref[0:1, :]) | (ids == slot_ref[1:2, :])
        chosen = jnp.where(hit, 1.0, 0.0).astype(jnp.bfloat16)
        xs[e] = jnp.dot(chosen, tok_ref[...], preferred_element_type=jnp.float32).astype(
            jnp.bfloat16
        )
        return carry

    lax.fori_loop(0, EXPERTS, pick, 0)
    for dz, dy in group:
        tokens_copy(dz, dy).start()
    xall[tp, arrived_rows(0, y), :] = xs[here]
    scale(1, u_ref)
    across(1)
    across(2)

    def turn(u):
        if u < len(SPLIT):
            m, lo, n = SPLIT[u]
            for dy in (1, 3, 2):
                ycopy(u, dy, yat(-dy)).wait_recv()
            away[m, pl.ds(lo, n), :] = ybuf[m, 1 - parity, :, lo : lo + n].T
            (og, ou)[m][z, pl.ds(lo, n), :] = ybuf[m, parity, :, lo : lo + n].T
        elif u == len(SPLIT):
            for part, (m, lo, n) in enumerate(DOWN):
                for dy in (1, 3, 2):
                    ycopy(u + part, dy, yat(-dy)).wait_recv()
                gone = ybuf[m, 1 - parity, :, lo : lo + n].T
                kept = ybuf[m, parity, :, lo : lo + n].T
                for f in range(2):
                    awayd[f, pl.ds(lo, n), :] = gone[:, f * LANES : (f + 1) * LANES]
                    od[f, z, pl.ds(lo, n), :] = kept[:, f * LANES : (f + 1) * LANES]

    def first(u, kinds=None):
        if kinds != "a":
            turn(u)
        for kind in kinds or ("ba" if u >= len(SPLIT) else "ab"):
            for sign in (1, -1):
                zcopy(u, kind, sign).start()

    def second(u, kinds="ab"):
        for kind in kinds:
            for sign in (1, -1):
                zcopy(u, kind, sign, True).wait_recv()
                zcopy(u, {"a": "c", "b": "d"}[kind], sign).start()

    def landed(u, kinds="cd"):
        for kind in kinds:
            for sign in (1, -1):
                zcopy(u, kind, sign, True).wait_recv()

    first(0)
    first(1)
    second(0)
    first(2)
    for dz, dy in group:
        tokens_copy(dz, dy, True).wait_recv()
    for step in (1, 3, 2):
        gather_copy(step).start()
    relay_copy(0).start()
    second(1)
    first(3)
    second(2)
    first(4)
    for step in (1, 3):
        gather_copy(step, True).wait_recv()
        relay_copy(step).start()
    second(3)
    gather_copy(2, True).wait_recv()
    relay_copy(2).start()
    second(4)
    first(5)
    first(6, "b")
    for step in range(NX):
        relay_copy(step, True).wait_recv()

    def norms(i, carry):
        at = pl.ds(pl.multiple_of(i * most, 16), most)
        total = jnp.zeros((most, 1), jnp.float32)
        for block in range(xall.shape[0]):
            v = xall[block, at, :].astype(jnp.float32)
            total = total + jnp.sum(v * v, axis=1, keepdims=True)
        mean = total / (xall.shape[0] * xall.shape[2])
        inv_ref[at, :] = lax.rsqrt(mean + epsilon)
        return carry

    lax.fori_loop(0, EXPERTS, norms, 0)
    for u in range(5):
        landed(u)

    tile = slots // 4

    def hide(i, carry):
        at = pl.ds(pl.multiple_of(i * tile, 16), tile)
        gate = jnp.zeros((tile, width), jnp.float32)
        up = jnp.zeros((tile, width), jnp.float32)
        for block in range(NZ):
            v = xall[block, at, :]
            gate = gate + lax.dot_general(v, og[block], ROWS, preferred_element_type=jnp.float32)
            up = up + lax.dot_general(v, ou[block], ROWS, preferred_element_type=jnp.float32)
        inverse = inv_ref[at, :]
        gate = gate * inverse
        up = up * inverse
        hidden[at, :] = (gate / (1.0 + jnp.exp(-gate)) * up).astype(jnp.bfloat16)
        return carry

    lax.fori_loop(0, slots // tile, hide, 0)
    second(5, "ba")
    first(6, "a")

    def block_at(k):
        return lax.rem(z + (2 * lax.rem(k, 2) - 1) * ((k + 1) // 2) + NZ, NZ)

    def half_rows(which):
        return pl.ds(pl.multiple_of(which * half_slots, 16), half_slots)

    def quarter_rows(which, q):
        return pl.ds(pl.multiple_of(which * half_slots + q * quarter, 16), quarter)

    bufs = (theirs, got, mine, joint, far)

    def pair_copy(k, f):
        at = f * NZ + k
        return pltpu.make_async_remote_copy(
            src_ref=bufs[0].at[at],
            dst_ref=bufs[1].at[at],
            send_sem=psend.at[at],
            recv_sem=precv.at[at],
            device_id=partner,
            device_id_type=MESH,
        )

    def home_copy(k, f):
        at = f * NZ + k
        return pltpu.make_async_remote_copy(
            src_ref=bufs[3].at[at],
            dst_ref=parts.at[0, half_rows(core), lanes(f)],
            send_sem=fsend.at[at * 2],
            recv_sem=rrecv.at[f * 9 + 8],
            device_id=partner,
            device_id_type=MESH,
        )

    def far_copy(k, f, q):
        at = f * NZ + k
        return pltpu.make_async_remote_copy(
            src_ref=bufs[3].at[at, pl.ds(q * quarter, quarter), :],
            dst_ref=bufs[4].at[at],
            send_sem=fsend.at[at * 2 + q],
            recv_sem=frecv.at[at * 2 + q],
            device_id=mate(1 - 2 * q),
            device_id_type=MESH,
        )

    def near_copy(k, f, q, side):
        at = f * NZ + k
        return pltpu.make_async_remote_copy(
            src_ref=bufs[3].at[at, pl.ds(q * quarter, quarter), :],
            dst_ref=parts.at[1 + side, quarter_rows(core, q), lanes(f)],
            send_sem=fsend.at[at * 2 + q],
            recv_sem=rrecv.at[f * 9 + side * 4 + core * 2 + q],
            device_id={"tp": block_at(k)},
            device_id_type=MESH,
        )

    def role(k):
        to = block_at(k)
        return to, lax.rem(to // 2 - x + NX, NX)

    def project(k, f):
        at = f * NZ + k
        weights = od[f, block_at(k)]
        bufs[0][at] = lax.dot_general(
            hidden[half_rows(1 - core), :], weights, COLS, preferred_element_type=jnp.float32
        ).astype(jnp.bfloat16)
        pair_copy(k, f).start()
        bufs[2][at] = lax.dot_general(
            hidden[half_rows(core), :], weights, COLS, preferred_element_type=jnp.float32
        ).astype(jnp.bfloat16)

    def project_two(k, f):
        at = f * NZ + k
        weights = jnp.concatenate([od[f, block_at(k)], od[f, block_at(k + 1)]], axis=1)
        for buf, which in ((0, 1 - core), (2, core)):
            value = lax.dot_general(
                hidden[half_rows(which), :], weights, COLS, preferred_element_type=jnp.float32
            ).astype(jnp.bfloat16)
            bufs[buf][at] = value[:, :LANES]
            bufs[buf][at + 1] = value[:, LANES:]
            if buf == 0:
                pair_copy(k, f).start()
                pair_copy(k + 1, f).start()

    def project_both(k):
        block = block_at(k)
        weights = jnp.concatenate([od[0, block], od[1, block]], axis=1)
        for buf, which in ((0, 1 - core), (2, core)):
            value = lax.dot_general(
                hidden[half_rows(which), :], weights, COLS, preferred_element_type=jnp.float32
            ).astype(jnp.bfloat16)
            for f in range(2):
                bufs[buf][f * NZ + k] = value[:, f * LANES : (f + 1) * LANES]
                if buf == 0:
                    pair_copy(k, f).start()

    def join(k, f):
        at = f * NZ + k
        to, which = role(k)
        pair_copy(k, f).wait_recv()
        bufs[3][at] = (
            bufs[2][at].astype(jnp.float32) + bufs[1][at].astype(jnp.float32)
        ).astype(jnp.bfloat16)

        @pl.when(to == tp)
        def _():
            parts[0, half_rows(core), lanes(f)] = bufs[3][at]

        @pl.when((which == 0) & (to != tp))
        def _():
            home_copy(k, f).start()

        @pl.when(which == 2)
        def _():
            far_copy(k, f, 0).start()
            far_copy(k, f, 1).start()

        @pl.when(which == 1)
        def _():
            near_copy(k, f, 1, 0).start()

        @pl.when(which == 3)
        def _():
            near_copy(k, f, 0, 1).start()

    def pass_on(k, f):
        at = f * NZ + k
        _, which = role(k)
        for when, q, side in ((1, 0, 0), (3, 1, 1)):

            @pl.when(which == when)
            def _():
                far_copy(k, f, q).wait_recv()
                piece = pl.ds(q * quarter, quarter)
                bufs[3][at, piece, :] = (
                    bufs[3][at, piece, :].astype(jnp.float32) + bufs[4][at].astype(jnp.float32)
                ).astype(jnp.bfloat16)
                near_copy(k, f, q, side).start()

    def sent(k, f):
        to, which = role(k)
        pair_copy(k, f).wait_send()

        @pl.when((which == 0) & (to != tp))
        def _():
            home_copy(k, f).wait_send()

        @pl.when(which != 0)
        def _():
            far_copy(k, f, 0).wait_send()
            far_copy(k, f, 1).wait_send()

    def near(f):
        project_two(0, f)
        project_two(2, f)
        join(0, f)
        join(1, f)
        project(4, f)
        for k in (2, 3, 4):
            join(k, f)

    def whole_wait(place, sem):
        pltpu.make_async_remote_copy(
            src_ref=place,
            dst_ref=place,
            send_sem=fsend.at[0],
            recv_sem=rrecv.at[sem],
            device_id=partner,
            device_id_type=MESH,
        ).wait_recv()

    def total(c, q, f):
        at = quarter_rows(c, q)
        value = parts[0, at, lanes(f)].astype(jnp.float32)
        for side in range(2):
            whole_wait(parts.at[1 + side, at, lanes(f)], f * 9 + side * 4 + c * 2 + q)
            value = value + parts[1 + side, at, lanes(f)].astype(jnp.float32)
        ret[at, lanes(f)] = value.astype(jnp.bfloat16)

    def give_back(f):
        whole_wait(parts.at[0, half_rows(1 - core), lanes(f)], f * 9 + 8)
        for q, dz in ((0, 1), (1, -1)):
            total(1, q, f)
            for dy in (0, 1, 3, 2):
                back_copy(dz, dy, f).start()
        total(0, 0, f)
        total(0, 1, f)
        for dy in (1, 3, 2):
            back_copy(0, dy, f).start()
        back[here, :, lanes(f)] = ret[arrived_rows(0, y), lanes(f)]

    def each(what, ks, f):
        for k in ks:
            what(k, f)

    close = range(NEAR)
    final = (NEAR, NEAR + 1)
    near(0)
    second(6, "b")
    landed(5, "d")
    project(NZ - 1, 0)
    join(NZ - 1, 0)
    each(pass_on, close, 0)
    landed(5, "c")
    project_two(NEAR, 0)
    each(join, final, 0)
    second(6, "a")
    near(1)
    each(pass_on, (NZ - 1, NEAR, NEAR + 1), 0)
    landed(6, "d")
    project(NZ - 1, 1)
    join(NZ - 1, 1)
    landed(6, "c")
    project_two(NEAR, 1)
    each(join, final, 1)
    each(pass_on, close, 1)
    pass_on(NZ - 1, 1)
    give_back(0)
    each(pass_on, final, 1)
    give_back(1)

    for f in range(2):
        for dz, dy in group:
            back_copy(dz, dy, f, True).wait_recv()

    count = tok_ref.shape[0]
    piece = count // 3

    def mix(i, carry):
        ids = lax.broadcasted_iota(jnp.int32, (piece, slots), 1)
        on = lax.broadcasted_iota(jnp.int32, (piece, count), 1) == (
            lax.broadcasted_iota(jnp.int32, (piece, count), 0) + i * piece
        )

        def column(line):
            return jnp.sum(jnp.where(on, line, 0.0), axis=1, keepdims=True)

        results = back[...].reshape(slots, back.shape[2])
        scores = [column(logit_ref[k : k + 1, :]) for k in range(2)]
        value = jnp.zeros((piece, back.shape[2]), jnp.float32)
        for k in range(2):
            wanted = column(slot_ref[k : k + 1, :].astype(jnp.float32)).astype(jnp.int32)
            chosen = jnp.where(ids == wanted, 1.0, 0.0).astype(jnp.bfloat16)
            picked = jnp.dot(chosen, results, preferred_element_type=jnp.float32)
            value = value + picked * jax.nn.sigmoid(scores[k] - scores[1 - k])
        mix_ref[pl.ds(pl.multiple_of(i * piece, 16), piece), :] = value.astype(jnp.bfloat16)
        return carry

    lax.fori_loop(0, count // piece, mix, 0)

    for u in range(UNITS):
        for dy in (1, 3, 2):
            ycopy(u, dy, y).wait_send()
        for kind in "abcd":
            for sign in (1, -1):
                zcopy(u, kind, sign).wait_send()
    for dz, dy in group:
        tokens_copy(dz, dy).wait_send()
        for f in range(2):
            back_copy(dz, dy, f).wait_send()
    for step in range(1, NX):
        gather_copy(step).wait_send()
    for step in range(NX):
        relay_copy(step).wait_send()
    for f in range(2):
        lax.fori_loop(0, NZ, lambda k, carry: (sent(k, f), carry)[1], 0)


def whole(gate, up, down, gain, tokens, routes, logits):
    _, rows, width = gate.shape
    count, features = tokens.shape
    most = count // 2
    split = [w.reshape(2, NY, rows, width) for w in (gate, up, down)]
    given = (*split, gain, tokens, routes, logits)
    bf16 = jnp.bfloat16
    out = jax.ShapeDtypeStruct((NZ, width, 2 * LANES), bf16)
    dma = lambda n: pltpu.SemaphoreType.DMA((n,))
    vmem = lambda *shape, dtype=bf16: pltpu.VMEM(shape, dtype)
    total = EXPERTS * most
    steps = 2 * NZ
    sums = [vmem(steps, total // 2, LANES)] * 4 + [vmem(steps, total // 4, LANES)]
    return pl.pallas_call(
        whole_kernel,
        out_shape=(
            out,
            out,
            jax.ShapeDtypeStruct((2, NZ, width, LANES), bf16),
            jax.ShapeDtypeStruct((count, features), bf16),
        ),
        in_specs=[pl.BlockSpec(memory_space=pltpu.HBM)] * 7,
        out_specs=(pl.BlockSpec(memory_space=pltpu.VMEM),) * 4,
        scratch_shapes=[
            *[pltpu.VMEM(a.shape, a.dtype) for a in given],
            vmem(2, 2, NY, rows, width),
            vmem(3, 2, NY * rows, width),
            vmem(2, width, 2 * LANES),
            vmem(2, width, LANES),
            vmem(8, count, dtype=jnp.int32),
            vmem(EXPERTS, most, features),
            vmem(2 * NX, total, features),
            vmem(total, 1, dtype=jnp.float32),
            vmem(total, width),
            *sums,
            vmem(3, total, features),
            vmem(total, features),
            vmem(EXPERTS, most, features),
            dma(3 * UNITS), dma(3 * UNITS), dma(8 * UNITS), dma(8 * UNITS),
            dma(3 * NY), dma(3 * NY), dma(2 * NX), dma(2 * NX),
            dma(steps), dma(steps), dma(2 * steps), dma(2 * steps), dma(18), dma(6 * NY), dma(6 * NY), dma(7),
        ],
        compiler_params=pltpu.CompilerParams(
            collective_id=0, has_side_effects=True, vmem_limit_bytes=VMEM_LIMIT
        ),
        cost_estimate=pl.CostEstimate(flops=10**11, bytes_accessed=10**7, transcendentals=0),
    )(*[pltpu.with_memory_space_constraint(a, pltpu.HBM) for a in given])


def place_kernel(g_ref, u_ref, d_ref, m_ref, og, ou, od, om, sem):
    copies = [pltpu.make_async_copy(m_ref, om, sem.at[4 * NZ])]
    for m, (ref, out) in enumerate(((g_ref, og), (u_ref, ou))):
        for block in range(NZ):
            columns = pl.ds(block * 2 * LANES, 2 * LANES)
            copies.append(
                pltpu.make_async_copy(ref.at[block], out.at[:, columns], sem.at[m * NZ + block])
            )
    for f in range(2):
        for block in range(NZ):
            columns = pl.ds((block * 2 + f) * LANES, LANES)
            at = (2 + f) * NZ + block
            copies.append(pltpu.make_async_copy(d_ref.at[f, block], od.at[:, columns], sem.at[at]))
    for copy in copies:
        copy.start()
    for copy in copies:
        copy.wait()


def placed_out(blocks):
    nz, width, size = blocks[0].shape
    out = jax.ShapeDtypeStruct((width, nz * size), jnp.bfloat16)
    *turned, mixed = pl.pallas_call(
        place_kernel,
        out_shape=(out, out, out, jax.ShapeDtypeStruct(blocks[3].shape, jnp.bfloat16)),
        in_specs=[pl.BlockSpec(memory_space=pltpu.VMEM)] * 4,
        out_specs=(pl.BlockSpec(memory_space=pl.ANY),) * 4,
        scratch_shapes=[pltpu.SemaphoreType.DMA((4 * NZ + 1,))],
        compiler_params=pltpu.CompilerParams(vmem_limit_bytes=2 * 1024 * 1024),
    )(*blocks)
    return (*[w.T[None] for w in turned], mixed)


def shards(tokens, norm_gain, gate_train, up_train, down_train, routes, route_logits):
    return placed_out(
        whole(
            gate_train, up_train, down_train, norm_gain[None, :], tokens, routes.T, route_logits.T
        )
    )


def solution(mesh):
    placed = (
        P("fs", "tp"),
        P("fs"),
        P(None, "fs", "tp"),
        P(None, "fs", "tp"),
        P(None, "fs", "tp"),
        P("fs", None),
        P("fs", None),
    )
    return jax.shard_map(
        shards,
        mesh=mesh,
        in_specs=placed,
        out_specs=(P("fs", None, "tp"), P("fs", None, "tp"), P("fs", None, "tp"), P("fs", "tp")),
        check_vma=False,
    )
```

```python
import functools

import jax
import jax.numpy as jnp
from jax import lax
from jax.experimental import pallas as pl
from jax.experimental.pallas import tpu as pltpu
from jax.sharding import PartitionSpec as P

EXPERTS = 8
epsilon = 1e-06
MESH = pl.DeviceIdType.MESH
NZ, NY = 8, 4
VMEM_LIMIT = 40 * 1024 * 1024
NZ, NY, NX = 8, 4, 4
LANES = 128
SPLIT = ((0, 0, 128), (0, 128, 256), (0, 384, 320), (1, 0, 384), (1, 384, 320))
DOWN = ((2, 0, 384), (2, 384, 320))
ACROSS = SPLIT + DOWN
UNITS = len(SPLIT) + 2
COLS = (((1,), (0,)), ((), ()))
ROWS = (((1,), (1,)), ((), ()))
NEAR = 5


def whole_kernel(
    g_in, u_in, d_in, gain_in, tok_in, route_in, logit_in,
    og, ou, od, mix_ref,
    g_ref, u_ref, d_ref, gain_ref, tok_ref, route_ref, logit_ref, scaled, ybuf, away, awayd, slot_ref, xs, xall, inv_ref, hidden,
    theirs, got, mine, joint, far, parts, ret, back, chosen_ref, share_ref,
    ysend, yrecv, zsend, zrecv, tsend, trecv, asend, arecv, psend, precv, fsend, frecv, rrecv, bsend, brecv, lsem,
):
    fs = lax.axis_index("fs")
    tp = lax.axis_index("tp")
    z, y = fs // NY, lax.rem(fs, NY)
    x, core = tp // 2, lax.rem(tp, 2)
    parity = lax.rem(z, 2)
    sources = (scaled.at[0], scaled.at[1], d_ref)
    rows = g_ref.shape[2]
    width = g_ref.shape[3]
    most = xs.shape[1]
    few = most // 2
    slots = xall.shape[1]
    half_slots = slots // 2
    quarter = slots // 4
    here = parity * NY + y

    def zat(step):
        return lax.rem(z + step + NZ, NZ)

    def yat(step):
        return lax.rem(y + step + NY, NY)

    def device(dz, dy):
        return {"fs": zat(dz) * NY + yat(dy)}

    def mate(step):
        return {"tp": lax.rem(x + step + NX, NX) * 2 + core}

    partner = {"tp": x * 2 + 1 - core}
    group = [(dz, dy) for dz, dys in ((1, (0, 1, 3, 2)), (-1, (0, 1, 3, 2)), (0, (1, 3, 2))) for dy in dys]

    loads = [
        pltpu.make_async_copy(source, held, lsem.at[i])
        for i, (source, held) in enumerate(
            (
                (g_in, g_ref),
                (gain_in, gain_ref),
                (route_in, route_ref),
                (tok_in, tok_ref),
                (u_in, u_ref),
                (d_in, d_ref),
                (logit_in, logit_ref),
            )
        )
    ]
    for load in loads:
        load.start()
    barrier = pltpu.get_barrier_semaphore()
    greeted = [device(dz, dy) for dz, dy in group + [(2, 0), (-2, 0)]]
    greeted += [{"tp": lax.rem(tp + step, 2 * NX)} for step in range(1, 2 * NX)]
    for other in greeted:
        pl.semaphore_signal(barrier, inc=1, device_id=other, device_id_type=MESH)

    def ycopy(u, dy, to_row):
        m, lo, n = ACROSS[u]
        return pltpu.make_async_remote_copy(
            src_ref=sources[m].at[:, yat(dy), :, pl.ds(lo, n)],
            dst_ref=ybuf.at[m, :, pl.ds(to_row * rows, rows), pl.ds(lo, n)],
            send_sem=ysend.at[u * 3 + dy - 1],
            recv_sem=yrecv.at[u * 3 + dy - 1],
            device_id=device(0, dy),
            device_id_type=MESH,
        )

    def zcopy(u, kind, sign, arriving=False):
        if u < len(SPLIT):
            m, lo, n = SPLIT[u]
            out, left = (og, ou)[m], away.at[m]
        else:
            lo, n = 0, width
            out, left = od.at[u - len(SPLIT)], awayd.at[u - len(SPLIT)]
        near = {"a": 1, "b": 2, "c": 2, "d": 2}[kind]
        hops = {"a": 0, "b": 0, "c": 1, "d": 2}[kind]
        block = zat(-sign * hops)
        if arriving:
            block = zat(-sign * (hops + near))
        if kind == "d":
            half = n // 2
            lo, n = (lo, half) if sign > 0 else (lo + half, half)
        place = out.at[block, pl.ds(lo, n), :]
        source = left.at[pl.ds(lo, n), :] if kind == "a" else place
        at = u * 8 + "abcd".index(kind) * 2 + (0 if sign > 0 else 1)
        return pltpu.make_async_remote_copy(
            src_ref=source,
            dst_ref=place,
            send_sem=zsend.at[at],
            recv_sem=zrecv.at[at],
            device_id=device(sign * near, 0),
            device_id_type=MESH,
        )

    def base(dz):
        return {0: 0, 1: half_slots, -1: half_slots + quarter}[dz]

    def arrived_rows(dz, at_y):
        n = few if dz else most
        return pl.ds(pl.multiple_of(base(dz) + at_y * n, 16), n)

    def held_rows(dz):
        return pl.ds({0: 0, 1: 0, -1: few}[dz], few if dz else most)

    def expert(dz, at_y):
        return ((1 - parity) if dz else parity) * NY + at_y

    def tokens_copy(dz, dy, arriving=False):
        at = (dz + 1) * NY + dy
        return pltpu.make_async_remote_copy(
            src_ref=xs.at[expert(dz, yat(dy)), held_rows(dz), :],
            dst_ref=xall.at[tp, arrived_rows(dz, yat(-dy) if arriving else y), :],
            send_sem=tsend.at[at],
            recv_sem=trecv.at[at],
            device_id=device(dz, dy),
            device_id_type=MESH,
        )

    def lanes(f):
        return pl.ds(f * LANES, LANES)

    def back_copy(dz, dy, f, arriving=False):
        at = (f * 3 + dz + 1) * NY + dy
        owner = expert(dz, yat(-dy)) if arriving else here
        return pltpu.make_async_remote_copy(
            src_ref=ret.at[arrived_rows(dz, yat(dy)), lanes(f)],
            dst_ref=back.at[owner, held_rows(dz), lanes(f)],
            send_sem=bsend.at[at],
            recv_sem=brecv.at[at],
            device_id=device(-dz, dy),
            device_id_type=MESH,
        )

    def gather_copy(step, arriving=False):
        block = lax.rem(x - step + NX, NX) * 2 + core if arriving else tp
        return pltpu.make_async_remote_copy(
            src_ref=xall.at[tp],
            dst_ref=xall.at[block],
            send_sem=asend.at[step],
            recv_sem=arecv.at[step],
            device_id=mate(step),
            device_id_type=MESH,
        )

    def relay_copy(step, arriving=False):
        block = lax.rem(x - step + NX, NX) * 2 + core
        if arriving:
            block = lax.rem(x - step + NX, NX) * 2 + 1 - core
        return pltpu.make_async_remote_copy(
            src_ref=xall.at[block],
            dst_ref=xall.at[block],
            send_sem=asend.at[NX + step],
            recv_sem=arecv.at[NX + step],
            device_id=partner,
            device_id_type=MESH,
        )

    def scale(m, ref):
        wide = gain_ref[...]
        on = lax.broadcasted_iota(jnp.int32, (rows, rows), 0) == lax.broadcasted_iota(
            jnp.int32, (rows, rows), 1
        )
        gain = jnp.sum(jnp.where(on, wide, 0.0), axis=1, keepdims=True)

        def one(e, carry):
            block = ref[e // NY, lax.rem(e, NY)]
            scaled[m, e // NY, lax.rem(e, NY)] = (block.astype(jnp.float32) * gain).astype(
                jnp.bfloat16
            )
            return carry

        lax.fori_loop(0, EXPERTS, one, 0)

    def across(m):
        for u, (owner, lo, n) in enumerate(ACROSS):
            if owner == m:
                for dy in (1, 3, 2):
                    ycopy(u, dy, y).start()
        ybuf[m, :, pl.ds(y * rows, rows), :] = sources[m][:, y]

    def plan():
        count = tok_ref.shape[0]
        lines = lax.broadcasted_iota(jnp.int32, (2 * EXPERTS, count), 0)
        routes = route_ref[...]
        named = (routes[0:1, :] == lines) | (routes[1:2, :] == lines - EXPERTS)
        named = jnp.where(named, 1.0, 0.0)
        before = jnp.where(
            lax.broadcasted_iota(jnp.int32, (count, count), 0)
            < lax.broadcasted_iota(jnp.int32, (count, count), 1),
            1.0,
            0.0,
        )
        rank = jnp.dot(
            named.astype(jnp.bfloat16),
            before.astype(jnp.bfloat16),
            preferred_element_type=jnp.float32,
        )
        for k in range(2):
            one = named[k * EXPERTS : (k + 1) * EXPERTS]
            place = rank[k * EXPERTS : (k + 1) * EXPERTS]
            if k:
                place = place + jnp.sum(named[:EXPERTS], axis=1, keepdims=True)
            place = place + (lines[:EXPERTS] * most).astype(jnp.float32)
            slot = jnp.sum(one * place, axis=0, keepdims=True)
            slot_ref[k : k + 1, :] = slot.astype(jnp.int32)

    for load in loads[:2]:
        load.wait()
    scale(0, g_ref)
    pl.semaphore_wait(barrier, len(greeted))
    across(0)
    for load in loads[2:]:
        load.wait()
    plan()

    def pick(e, carry):
        ids = lax.broadcasted_iota(jnp.int32, (most, tok_ref.shape[0]), 0) + e * most
        hit = (ids == slot_ref[0:1, :]) | (ids == slot_ref[1:2, :])
        chosen = jnp.where(hit, 1.0, 0.0).astype(jnp.bfloat16)
        xs[e] = jnp.dot(chosen, tok_ref[...], preferred_element_type=jnp.float32).astype(
            jnp.bfloat16
        )
        return carry

    lax.fori_loop(0, EXPERTS, pick, 0)
    for dz, dy in group:
        tokens_copy(dz, dy).start()
    xall[tp, arrived_rows(0, y), :] = xs[here]
    scale(1, u_ref)
    across(1)
    across(2)

    def turn(u):
        if u < len(SPLIT):
            m, lo, n = SPLIT[u]
            for dy in (1, 3, 2):
                ycopy(u, dy, yat(-dy)).wait_recv()
            away[m, pl.ds(lo, n), :] = ybuf[m, 1 - parity, :, lo : lo + n].T
            (og, ou)[m][z, pl.ds(lo, n), :] = ybuf[m, parity, :, lo : lo + n].T
        elif u == len(SPLIT):
            for part, (m, lo, n) in enumerate(DOWN):
                for dy in (1, 3, 2):
                    ycopy(u + part, dy, yat(-dy)).wait_recv()
                gone = ybuf[m, 1 - parity, :, lo : lo + n].T
                kept = ybuf[m, parity, :, lo : lo + n].T
                for f in range(2):
                    awayd[f, pl.ds(lo, n), :] = gone[:, f * LANES : (f + 1) * LANES]
                    od[f, z, pl.ds(lo, n), :] = kept[:, f * LANES : (f + 1) * LANES]

    def first(u, kinds=None):
        if kinds != "a":
            turn(u)
        for kind in kinds or ("ba" if u >= len(SPLIT) else "ab"):
            for sign in (1, -1):
                zcopy(u, kind, sign).start()

    def second(u, kinds="ab"):
        for kind in kinds:
            for sign in (1, -1):
                zcopy(u, kind, sign, True).wait_recv()
                zcopy(u, {"a": "c", "b": "d"}[kind], sign).start()

    def landed(u, kinds="cd"):
        for kind in kinds:
            for sign in (1, -1):
                zcopy(u, kind, sign, True).wait_recv()

    first(0)
    first(1)
    second(0)
    first(2)
    for dz, dy in group:
        tokens_copy(dz, dy, True).wait_recv()
    for step in (1, 3, 2):
        gather_copy(step).start()
    relay_copy(0).start()
    second(1)
    first(3)
    second(2)
    first(4)
    for step in (1, 3):
        gather_copy(step, True).wait_recv()
        relay_copy(step).start()
    second(3)
    gather_copy(2, True).wait_recv()
    relay_copy(2).start()
    second(4)
    first(5)
    first(6, "b")
    for step in range(NX):
        relay_copy(step, True).wait_recv()

    def norms(i, carry):
        at = pl.ds(pl.multiple_of(i * most, 16), most)
        total = jnp.zeros((most, 1), jnp.float32)
        for block in range(xall.shape[0]):
            v = xall[block, at, :].astype(jnp.float32)
            total = total + jnp.sum(v * v, axis=1, keepdims=True)
        mean = total / (xall.shape[0] * xall.shape[2])
        inv_ref[at, :] = lax.rsqrt(mean + epsilon)
        return carry

    lax.fori_loop(0, EXPERTS, norms, 0)

    count = tok_ref.shape[0]
    piece = count // 3

    def choose(i, carry):
        at = pl.ds(pl.multiple_of(i * piece, 16), piece)
        ids = lax.broadcasted_iota(jnp.int32, (piece, slots), 1)
        on = lax.broadcasted_iota(jnp.int32, (piece, count), 1) == (
            lax.broadcasted_iota(jnp.int32, (piece, count), 0) + i * piece
        )

        def column(line):
            return jnp.sum(jnp.where(on, line, 0.0), axis=1, keepdims=True)

        scores = [column(logit_ref[k : k + 1, :]) for k in range(2)]
        for k in range(2):
            wanted = column(slot_ref[k : k + 1, :].astype(jnp.float32)).astype(jnp.int32)
            chosen_ref[k, at, :] = jnp.where(ids == wanted, 1.0, 0.0).astype(jnp.bfloat16)
            share_ref[at, k : k + 1] = jax.nn.sigmoid(scores[k] - scores[1 - k])
        return carry

    lax.fori_loop(0, count // piece, choose, 0)
    for u in range(5):
        landed(u)

    tile = slots // 4

    def hide(i, carry):
        at = pl.ds(pl.multiple_of(i * tile, 16), tile)
        gate = jnp.zeros((tile, width), jnp.float32)
        up = jnp.zeros((tile, width), jnp.float32)
        for block in range(NZ):
            v = xall[block, at, :]
            gate = gate + lax.dot_general(v, og[block], ROWS, preferred_element_type=jnp.float32)
            up = up + lax.dot_general(v, ou[block], ROWS, preferred_element_type=jnp.float32)
        inverse = inv_ref[at, :]
        gate = gate * inverse
        up = up * inverse
        hidden[at, :] = (gate / (1.0 + jnp.exp(-gate)) * up).astype(jnp.bfloat16)
        return carry

    lax.fori_loop(0, slots // tile, hide, 0)
    second(5, "ba")
    first(6, "a")

    def block_at(k):
        return lax.rem(z + (2 * lax.rem(k, 2) - 1) * ((k + 1) // 2) + NZ, NZ)

    def half_rows(which):
        return pl.ds(pl.multiple_of(which * half_slots, 16), half_slots)

    def quarter_rows(which, q):
        return pl.ds(pl.multiple_of(which * half_slots + q * quarter, 16), quarter)

    bufs = (theirs, got, mine, joint, far)

    def pair_copy(k, f):
        at = f * NZ + k
        return pltpu.make_async_remote_copy(
            src_ref=bufs[0].at[at],
            dst_ref=bufs[1].at[at],
            send_sem=psend.at[at],
            recv_sem=precv.at[at],
            device_id=partner,
            device_id_type=MESH,
        )

    def home_copy(k, f):
        at = f * NZ + k
        return pltpu.make_async_remote_copy(
            src_ref=bufs[3].at[at],
            dst_ref=parts.at[0, half_rows(core), lanes(f)],
            send_sem=fsend.at[at * 2],
            recv_sem=rrecv.at[f * 9 + 8],
            device_id=partner,
            device_id_type=MESH,
        )

    def far_copy(k, f, q):
        at = f * NZ + k
        return pltpu.make_async_remote_copy(
            src_ref=bufs[3].at[at, pl.ds(q * quarter, quarter), :],
            dst_ref=bufs[4].at[at],
            send_sem=fsend.at[at * 2 + q],
            recv_sem=frecv.at[at * 2 + q],
            device_id=mate(1 - 2 * q),
            device_id_type=MESH,
        )

    def near_copy(k, f, q, side):
        at = f * NZ + k
        return pltpu.make_async_remote_copy(
            src_ref=bufs[3].at[at, pl.ds(q * quarter, quarter), :],
            dst_ref=parts.at[1 + side, quarter_rows(core, q), lanes(f)],
            send_sem=fsend.at[at * 2 + q],
            recv_sem=rrecv.at[f * 9 + side * 4 + core * 2 + q],
            device_id={"tp": block_at(k)},
            device_id_type=MESH,
        )

    def role(k):
        to = block_at(k)
        return to, lax.rem(to // 2 - x + NX, NX)

    def project(k, f):
        at = f * NZ + k
        weights = od[f, block_at(k)]
        bufs[0][at] = lax.dot_general(
            hidden[half_rows(1 - core), :], weights, COLS, preferred_element_type=jnp.float32
        ).astype(jnp.bfloat16)
        pair_copy(k, f).start()
        bufs[2][at] = lax.dot_general(
            hidden[half_rows(core), :], weights, COLS, preferred_element_type=jnp.float32
        ).astype(jnp.bfloat16)

    def project_two(k, f):
        at = f * NZ + k
        weights = jnp.concatenate([od[f, block_at(k)], od[f, block_at(k + 1)]], axis=1)
        for buf, which in ((0, 1 - core), (2, core)):
            value = lax.dot_general(
                hidden[half_rows(which), :], weights, COLS, preferred_element_type=jnp.float32
            ).astype(jnp.bfloat16)
            bufs[buf][at] = value[:, :LANES]
            bufs[buf][at + 1] = value[:, LANES:]
            if buf == 0:
                pair_copy(k, f).start()
                pair_copy(k + 1, f).start()

    def project_both(k):
        block = block_at(k)
        weights = jnp.concatenate([od[0, block], od[1, block]], axis=1)
        for buf, which in ((0, 1 - core), (2, core)):
            value = lax.dot_general(
                hidden[half_rows(which), :], weights, COLS, preferred_element_type=jnp.float32
            ).astype(jnp.bfloat16)
            for f in range(2):
                bufs[buf][f * NZ + k] = value[:, f * LANES : (f + 1) * LANES]
                if buf == 0:
                    pair_copy(k, f).start()

    def join(k, f):
        at = f * NZ + k
        to, which = role(k)
        pair_copy(k, f).wait_recv()
        bufs[3][at] = (
            bufs[2][at].astype(jnp.float32) + bufs[1][at].astype(jnp.float32)
        ).astype(jnp.bfloat16)

        @pl.when(to == tp)
        def _():
            parts[0, half_rows(core), lanes(f)] = bufs[3][at]

        @pl.when((which == 0) & (to != tp))
        def _():
            home_copy(k, f).start()

        @pl.when(which == 2)
        def _():
            far_copy(k, f, 0).start()
            far_copy(k, f, 1).start()

        @pl.when(which == 1)
        def _():
            near_copy(k, f, 1, 0).start()

        @pl.when(which == 3)
        def _():
            near_copy(k, f, 0, 1).start()

    def pass_on(k, f):
        at = f * NZ + k
        _, which = role(k)
        for when, q, side in ((1, 0, 0), (3, 1, 1)):

            @pl.when(which == when)
            def _():
                far_copy(k, f, q).wait_recv()
                piece = pl.ds(q * quarter, quarter)
                bufs[3][at, piece, :] = (
                    bufs[3][at, piece, :].astype(jnp.float32) + bufs[4][at].astype(jnp.float32)
                ).astype(jnp.bfloat16)
                near_copy(k, f, q, side).start()

    def sent(k, f):
        to, which = role(k)
        pair_copy(k, f).wait_send()

        @pl.when((which == 0) & (to != tp))
        def _():
            home_copy(k, f).wait_send()

        @pl.when(which != 0)
        def _():
            far_copy(k, f, 0).wait_send()
            far_copy(k, f, 1).wait_send()

    def near(f):
        project_two(0, f)
        project_two(2, f)
        join(0, f)
        join(1, f)
        project(4, f)
        for k in (2, 3, 4):
            join(k, f)

    def whole_wait(place, sem):
        pltpu.make_async_remote_copy(
            src_ref=place,
            dst_ref=place,
            send_sem=fsend.at[0],
            recv_sem=rrecv.at[sem],
            device_id=partner,
            device_id_type=MESH,
        ).wait_recv()

    def total(c, q, f):
        at = quarter_rows(c, q)
        value = parts[0, at, lanes(f)].astype(jnp.float32)
        for side in range(2):
            whole_wait(parts.at[1 + side, at, lanes(f)], f * 9 + side * 4 + c * 2 + q)
            value = value + parts[1 + side, at, lanes(f)].astype(jnp.float32)
        ret[at, lanes(f)] = value.astype(jnp.bfloat16)

    def give_back(f):
        whole_wait(parts.at[0, half_rows(1 - core), lanes(f)], f * 9 + 8)
        for q, dz in ((0, 1), (1, -1)):
            total(1, q, f)
            for dy in (0, 1, 3, 2):
                back_copy(dz, dy, f).start()
        total(0, 0, f)
        total(0, 1, f)
        for dy in (1, 3, 2):
            back_copy(0, dy, f).start()
        back[here, :, lanes(f)] = ret[arrived_rows(0, y), lanes(f)]

    def each(what, ks, f):
        for k in ks:
            what(k, f)

    close = range(NEAR)
    final = (NEAR, NEAR + 1)
    near(0)
    second(6, "b")
    landed(5, "d")
    project(NZ - 1, 0)
    join(NZ - 1, 0)
    each(pass_on, close, 0)
    landed(5, "c")
    project_two(NEAR, 0)
    each(join, final, 0)
    second(6, "a")
    near(1)
    each(pass_on, (NZ - 1, NEAR, NEAR + 1), 0)
    landed(6, "d")
    project(NZ - 1, 1)
    join(NZ - 1, 1)
    landed(6, "c")
    project_two(NEAR, 1)
    each(join, final, 1)
    each(pass_on, close, 1)
    pass_on(NZ - 1, 1)
    give_back(0)
    each(pass_on, final, 1)
    give_back(1)

    def mix(f):
        def one(i, carry):
            at = pl.ds(pl.multiple_of(i * piece, 16), piece)
            results = back[:, :, lanes(f)].reshape(slots, LANES)
            value = jnp.zeros((piece, LANES), jnp.float32)
            for k in range(2):
                picked = jnp.dot(
                    chosen_ref[k, at, :], results, preferred_element_type=jnp.float32
                )
                value = value + picked * share_ref[at, k : k + 1]
            mix_ref[at, lanes(f)] = value.astype(jnp.bfloat16)
            return carry

        lax.fori_loop(0, count // piece, one, 0)

    for f in range(2):
        for dz, dy in group:
            back_copy(dz, dy, f, True).wait_recv()
        mix(f)

    for u in range(UNITS):
        for dy in (1, 3, 2):
            ycopy(u, dy, y).wait_send()
        for kind in "abcd":
            for sign in (1, -1):
                zcopy(u, kind, sign).wait_send()
    for dz, dy in group:
        tokens_copy(dz, dy).wait_send()
        for f in range(2):
            back_copy(dz, dy, f).wait_send()
    for step in range(1, NX):
        gather_copy(step).wait_send()
    for step in range(NX):
        relay_copy(step).wait_send()
    for f in range(2):
        lax.fori_loop(0, NZ, lambda k, carry: (sent(k, f), carry)[1], 0)


def whole(gate, up, down, gain, tokens, routes, logits):
    _, rows, width = gate.shape
    count, features = tokens.shape
    most = count // 2
    split = [w.reshape(2, NY, rows, width) for w in (gate, up, down)]
    given = (*split, gain, tokens, routes, logits)
    bf16 = jnp.bfloat16
    out = jax.ShapeDtypeStruct((NZ, width, 2 * LANES), bf16)
    dma = lambda n: pltpu.SemaphoreType.DMA((n,))
    vmem = lambda *shape, dtype=bf16: pltpu.VMEM(shape, dtype)
    total = EXPERTS * most
    steps = 2 * NZ
    sums = [vmem(steps, total // 2, LANES)] * 4 + [vmem(steps, total // 4, LANES)]
    return pl.pallas_call(
        whole_kernel,
        out_shape=(
            out,
            out,
            jax.ShapeDtypeStruct((2, NZ, width, LANES), bf16),
            jax.ShapeDtypeStruct((count, features), bf16),
        ),
        in_specs=[pl.BlockSpec(memory_space=pltpu.HBM)] * 7,
        out_specs=(pl.BlockSpec(memory_space=pltpu.VMEM),) * 4,
        scratch_shapes=[
            *[pltpu.VMEM(a.shape, a.dtype) for a in given],
            vmem(2, 2, NY, rows, width),
            vmem(3, 2, NY * rows, width),
            vmem(2, width, 2 * LANES),
            vmem(2, width, LANES),
            vmem(8, count, dtype=jnp.int32),
            vmem(EXPERTS, most, features),
            vmem(2 * NX, total, features),
            vmem(total, 1, dtype=jnp.float32),
            vmem(total, width),
            *sums,
            vmem(3, total, features),
            vmem(total, features),
            vmem(EXPERTS, most, features),
            vmem(2, count, total),
            vmem(count, LANES, dtype=jnp.float32),
            dma(3 * UNITS), dma(3 * UNITS), dma(8 * UNITS), dma(8 * UNITS),
            dma(3 * NY), dma(3 * NY), dma(2 * NX), dma(2 * NX),
            dma(steps), dma(steps), dma(2 * steps), dma(2 * steps), dma(18), dma(6 * NY), dma(6 * NY), dma(7),
        ],
        compiler_params=pltpu.CompilerParams(
            collective_id=0, has_side_effects=True, vmem_limit_bytes=VMEM_LIMIT
        ),
        cost_estimate=pl.CostEstimate(flops=10**11, bytes_accessed=10**7, transcendentals=0),
    )(*[pltpu.with_memory_space_constraint(a, pltpu.HBM) for a in given])


def place_kernel(g_ref, u_ref, d_ref, m_ref, og, ou, od, om, sem):
    copies = [pltpu.make_async_copy(m_ref, om, sem.at[4 * NZ])]
    for m, (ref, out) in enumerate(((g_ref, og), (u_ref, ou))):
        for block in range(NZ):
            columns = pl.ds(block * 2 * LANES, 2 * LANES)
            copies.append(
                pltpu.make_async_copy(ref.at[block], out.at[:, columns], sem.at[m * NZ + block])
            )
    for f in range(2):
        for block in range(NZ):
            columns = pl.ds((block * 2 + f) * LANES, LANES)
            at = (2 + f) * NZ + block
            copies.append(pltpu.make_async_copy(d_ref.at[f, block], od.at[:, columns], sem.at[at]))
    for copy in copies:
        copy.start()
    for copy in copies:
        copy.wait()


def placed_out(blocks):
    nz, width, size = blocks[0].shape
    out = jax.ShapeDtypeStruct((width, nz * size), jnp.bfloat16)
    *turned, mixed = pl.pallas_call(
        place_kernel,
        out_shape=(out, out, out, jax.ShapeDtypeStruct(blocks[3].shape, jnp.bfloat16)),
        in_specs=[pl.BlockSpec(memory_space=pltpu.VMEM)] * 4,
        out_specs=(pl.BlockSpec(memory_space=pl.ANY),) * 4,
        scratch_shapes=[pltpu.SemaphoreType.DMA((4 * NZ + 1,))],
        compiler_params=pltpu.CompilerParams(vmem_limit_bytes=2 * 1024 * 1024),
    )(*blocks)
    return (*[w.T[None] for w in turned], mixed)


def shards(tokens, norm_gain, gate_train, up_train, down_train, routes, route_logits):
    return placed_out(
        whole(
            gate_train, up_train, down_train, norm_gain[None, :], tokens, routes.T, route_logits.T
        )
    )


def solution(mesh):
    placed = (
        P("fs", "tp"),
        P("fs"),
        P(None, "fs", "tp"),
        P(None, "fs", "tp"),
        P(None, "fs", "tp"),
        P("fs", None),
        P("fs", None),
    )
    return jax.shard_map(
        shards,
        mesh=mesh,
        in_specs=placed,
        out_specs=(P("fs", None, "tp"), P("fs", None, "tp"), P("fs", None, "tp"), P("fs", "tp")),
        check_vma=False,
    )
```

```python
import functools

import jax
import jax.numpy as jnp
from jax import lax
from jax.experimental import pallas as pl
from jax.experimental.pallas import tpu as pltpu
from jax.sharding import PartitionSpec as P

EXPERTS = 8
epsilon = 1e-06
MESH = pl.DeviceIdType.MESH
NZ, NY = 8, 4
VMEM_LIMIT = 40 * 1024 * 1024
NZ, NY, NX = 8, 4, 4
LANES = 128
SPLIT = ((0, 0, 128), (0, 128, 128), (0, 256, 448), (1, 0, 384), (1, 384, 320))
DOWN = ((2, 0, 384), (2, 384, 320))
ACROSS = SPLIT + DOWN
UNITS = len(SPLIT) + 2
COLS = (((1,), (0,)), ((), ()))
ROWS = (((1,), (1,)), ((), ()))
NEAR = 5


def whole_kernel(
    g_in, u_in, d_in, gain_in, tok_in, route_in, logit_in,
    og, ou, od, mix_ref,
    g_ref, u_ref, d_ref, gain_ref, tok_ref, route_ref, logit_ref, scaled, ybuf, away, awayd, slot_ref, xs, xall, inv_ref, hidden,
    theirs, got, mine, joint, far, parts, ret, back, chosen_ref, share_ref,
    ysend, yrecv, zsend, zrecv, tsend, trecv, asend, arecv, psend, precv, fsend, frecv, rrecv, bsend, brecv, lsem,
):
    fs = lax.axis_index("fs")
    tp = lax.axis_index("tp")
    z, y = fs // NY, lax.rem(fs, NY)
    x, core = tp // 2, lax.rem(tp, 2)
    parity = lax.rem(z, 2)
    sources = (scaled.at[0], scaled.at[1], d_ref)
    rows = g_ref.shape[2]
    width = g_ref.shape[3]
    most = xs.shape[1]
    few = most // 2
    slots = xall.shape[1]
    half_slots = slots // 2
    quarter = slots // 4
    here = parity * NY + y

    def zat(step):
        return lax.rem(z + step + NZ, NZ)

    def yat(step):
        return lax.rem(y + step + NY, NY)

    def device(dz, dy):
        return {"fs": zat(dz) * NY + yat(dy)}

    def mate(step):
        return {"tp": lax.rem(x + step + NX, NX) * 2 + core}

    partner = {"tp": x * 2 + 1 - core}
    group = [(dz, dy) for dz, dys in ((1, (0, 1, 3, 2)), (-1, (0, 1, 3, 2)), (0, (1, 3, 2))) for dy in dys]

    loads = [
        pltpu.make_async_copy(source, held, lsem.at[i])
        for i, (source, held) in enumerate(
            (
                (g_in, g_ref),
                (gain_in, gain_ref),
                (route_in, route_ref),
                (tok_in, tok_ref),
                (u_in, u_ref),
                (d_in, d_ref),
                (logit_in, logit_ref),
            )
        )
    ]
    for load in loads:
        load.start()
    barrier = pltpu.get_barrier_semaphore()
    greeted = [device(dz, dy) for dz, dy in group + [(2, 0), (-2, 0)]]
    greeted += [{"tp": lax.rem(tp + step, 2 * NX)} for step in range(1, 2 * NX)]
    for other in greeted:
        pl.semaphore_signal(barrier, inc=1, device_id=other, device_id_type=MESH)

    def ycopy(u, dy, to_row):
        m, lo, n = ACROSS[u]
        return pltpu.make_async_remote_copy(
            src_ref=sources[m].at[:, yat(dy), :, pl.ds(lo, n)],
            dst_ref=ybuf.at[m, :, pl.ds(to_row * rows, rows), pl.ds(lo, n)],
            send_sem=ysend.at[u * 3 + dy - 1],
            recv_sem=yrecv.at[u * 3 + dy - 1],
            device_id=device(0, dy),
            device_id_type=MESH,
        )

    def zcopy(u, kind, sign, arriving=False):
        if u < len(SPLIT):
            m, lo, n = SPLIT[u]
            out, left = (og, ou)[m], away.at[m]
        else:
            lo, n = 0, width
            out, left = od.at[u - len(SPLIT)], awayd.at[u - len(SPLIT)]
        near = {"a": 1, "b": 2, "c": 2, "d": 2}[kind]
        hops = {"a": 0, "b": 0, "c": 1, "d": 2}[kind]
        block = zat(-sign * hops)
        if arriving:
            block = zat(-sign * (hops + near))
        if kind == "d":
            half = n // 2
            lo, n = (lo, half) if sign > 0 else (lo + half, half)
        place = out.at[block, pl.ds(lo, n), :]
        source = left.at[pl.ds(lo, n), :] if kind == "a" else place
        at = u * 8 + "abcd".index(kind) * 2 + (0 if sign > 0 else 1)
        return pltpu.make_async_remote_copy(
            src_ref=source,
            dst_ref=place,
            send_sem=zsend.at[at],
            recv_sem=zrecv.at[at],
            device_id=device(sign * near, 0),
            device_id_type=MESH,
        )

    def base(dz):
        return {0: 0, 1: half_slots, -1: half_slots + quarter}[dz]

    def arrived_rows(dz, at_y):
        n = few if dz else most
        return pl.ds(pl.multiple_of(base(dz) + at_y * n, 16), n)

    def held_rows(dz):
        return pl.ds({0: 0, 1: 0, -1: few}[dz], few if dz else most)

    def expert(dz, at_y):
        return ((1 - parity) if dz else parity) * NY + at_y

    def tokens_copy(dz, dy, arriving=False):
        at = (dz + 1) * NY + dy
        return pltpu.make_async_remote_copy(
            src_ref=xs.at[expert(dz, yat(dy)), held_rows(dz), :],
            dst_ref=xall.at[tp, arrived_rows(dz, yat(-dy) if arriving else y), :],
            send_sem=tsend.at[at],
            recv_sem=trecv.at[at],
            device_id=device(dz, dy),
            device_id_type=MESH,
        )

    def lanes(f):
        return pl.ds(f * LANES, LANES)

    def back_copy(dz, dy, f, arriving=False):
        at = (f * 3 + dz + 1) * NY + dy
        owner = expert(dz, yat(-dy)) if arriving else here
        return pltpu.make_async_remote_copy(
            src_ref=ret.at[arrived_rows(dz, yat(dy)), lanes(f)],
            dst_ref=back.at[owner, held_rows(dz), lanes(f)],
            send_sem=bsend.at[at],
            recv_sem=brecv.at[at],
            device_id=device(-dz, dy),
            device_id_type=MESH,
        )

    def gather_copy(step, arriving=False):
        block = lax.rem(x - step + NX, NX) * 2 + core if arriving else tp
        return pltpu.make_async_remote_copy(
            src_ref=xall.at[tp],
            dst_ref=xall.at[block],
            send_sem=asend.at[step],
            recv_sem=arecv.at[step],
            device_id=mate(step),
            device_id_type=MESH,
        )

    def relay_copy(step, arriving=False):
        block = lax.rem(x - step + NX, NX) * 2 + core
        if arriving:
            block = lax.rem(x - step + NX, NX) * 2 + 1 - core
        return pltpu.make_async_remote_copy(
            src_ref=xall.at[block],
            dst_ref=xall.at[block],
            send_sem=asend.at[NX + step],
            recv_sem=arecv.at[NX + step],
            device_id=partner,
            device_id_type=MESH,
        )

    def scale(m, ref):
        wide = gain_ref[...]
        on = lax.broadcasted_iota(jnp.int32, (rows, rows), 0) == lax.broadcasted_iota(
            jnp.int32, (rows, rows), 1
        )
        gain = jnp.sum(jnp.where(on, wide, 0.0), axis=1, keepdims=True)

        def one(e, carry):
            block = ref[e // NY, lax.rem(e, NY)]
            scaled[m, e // NY, lax.rem(e, NY)] = (block.astype(jnp.float32) * gain).astype(
                jnp.bfloat16
            )
            return carry

        lax.fori_loop(0, EXPERTS, one, 0)

    def across(m):
        for u, (owner, lo, n) in enumerate(ACROSS):
            if owner == m:
                for dy in (1, 3, 2):
                    ycopy(u, dy, y).start()
        ybuf[m, :, pl.ds(y * rows, rows), :] = sources[m][:, y]

    def plan():
        count = tok_ref.shape[0]
        lines = lax.broadcasted_iota(jnp.int32, (2 * EXPERTS, count), 0)
        routes = route_ref[...]
        named = (routes[0:1, :] == lines) | (routes[1:2, :] == lines - EXPERTS)
        named = jnp.where(named, 1.0, 0.0)
        before = jnp.where(
            lax.broadcasted_iota(jnp.int32, (count, count), 0)
            < lax.broadcasted_iota(jnp.int32, (count, count), 1),
            1.0,
            0.0,
        )
        rank = jnp.dot(
            named.astype(jnp.bfloat16),
            before.astype(jnp.bfloat16),
            preferred_element_type=jnp.float32,
        )
        for k in range(2):
            one = named[k * EXPERTS : (k + 1) * EXPERTS]
            place = rank[k * EXPERTS : (k + 1) * EXPERTS]
            if k:
                place = place + jnp.sum(named[:EXPERTS], axis=1, keepdims=True)
            place = place + (lines[:EXPERTS] * most).astype(jnp.float32)
            slot = jnp.sum(one * place, axis=0, keepdims=True)
            slot_ref[k : k + 1, :] = slot.astype(jnp.int32)

    for load in loads[:2]:
        load.wait()
    scale(0, g_ref)
    pl.semaphore_wait(barrier, len(greeted))
    across(0)
    for load in loads[2:]:
        load.wait()
    plan()

    def pick(e, carry):
        ids = lax.broadcasted_iota(jnp.int32, (most, tok_ref.shape[0]), 0) + e * most
        hit = (ids == slot_ref[0:1, :]) | (ids == slot_ref[1:2, :])
        chosen = jnp.where(hit, 1.0, 0.0).astype(jnp.bfloat16)
        xs[e] = jnp.dot(chosen, tok_ref[...], preferred_element_type=jnp.float32).astype(
            jnp.bfloat16
        )
        return carry

    lax.fori_loop(0, EXPERTS, pick, 0)
    for dz, dy in group:
        tokens_copy(dz, dy).start()
    xall[tp, arrived_rows(0, y), :] = xs[here]
    scale(1, u_ref)
    across(1)
    across(2)

    def turn(u):
        if u < len(SPLIT):
            m, lo, n = SPLIT[u]
            for dy in (1, 3, 2):
                ycopy(u, dy, yat(-dy)).wait_recv()
            away[m, pl.ds(lo, n), :] = ybuf[m, 1 - parity, :, lo : lo + n].T
            (og, ou)[m][z, pl.ds(lo, n), :] = ybuf[m, parity, :, lo : lo + n].T
        elif u == len(SPLIT):
            for part, (m, lo, n) in enumerate(DOWN):
                for dy in (1, 3, 2):
                    ycopy(u + part, dy, yat(-dy)).wait_recv()
                gone = ybuf[m, 1 - parity, :, lo : lo + n].T
                kept = ybuf[m, parity, :, lo : lo + n].T
                for f in range(2):
                    awayd[f, pl.ds(lo, n), :] = gone[:, f * LANES : (f + 1) * LANES]
                    od[f, z, pl.ds(lo, n), :] = kept[:, f * LANES : (f + 1) * LANES]

    def first(u, kinds=None):
        if kinds != "a":
            turn(u)
        for kind in kinds or ("ba" if u >= len(SPLIT) else "ab"):
            for sign in (1, -1):
                zcopy(u, kind, sign).start()

    def second(u, kinds="ab"):
        for kind in kinds:
            for sign in (1, -1):
                zcopy(u, kind, sign, True).wait_recv()
                zcopy(u, {"a": "c", "b": "d"}[kind], sign).start()

    def landed(u, kinds="cd"):
        for kind in kinds:
            for sign in (1, -1):
                zcopy(u, kind, sign, True).wait_recv()

    first(0)
    first(1)
    second(0)
    first(2)
    for dz, dy in group:
        tokens_copy(dz, dy, True).wait_recv()
    for step in (1, 3, 2):
        gather_copy(step).start()
    relay_copy(0).start()
    second(1)
    first(3)
    second(2)
    first(4)
    for step in (1, 3):
        gather_copy(step, True).wait_recv()
        relay_copy(step).start()
    second(3)
    gather_copy(2, True).wait_recv()
    relay_copy(2).start()
    second(4)
    first(5)
    first(6, "b")
    for step in range(NX):
        relay_copy(step, True).wait_recv()

    def norms(i, carry):
        at = pl.ds(pl.multiple_of(i * most, 16), most)
        total = jnp.zeros((most, 1), jnp.float32)
        for block in range(xall.shape[0]):
            v = xall[block, at, :].astype(jnp.float32)
            total = total + jnp.sum(v * v, axis=1, keepdims=True)
        mean = total / (xall.shape[0] * xall.shape[2])
        inv_ref[at, :] = lax.rsqrt(mean + epsilon)
        return carry

    lax.fori_loop(0, EXPERTS, norms, 0)

    count = tok_ref.shape[0]
    piece = count // 3

    def choose(i, carry):
        at = pl.ds(pl.multiple_of(i * piece, 16), piece)
        ids = lax.broadcasted_iota(jnp.int32, (piece, slots), 1)
        on = lax.broadcasted_iota(jnp.int32, (piece, count), 1) == (
            lax.broadcasted_iota(jnp.int32, (piece, count), 0) + i * piece
        )

        def column(line):
            return jnp.sum(jnp.where(on, line, 0.0), axis=1, keepdims=True)

        scores = [column(logit_ref[k : k + 1, :]) for k in range(2)]
        for k in range(2):
            wanted = column(slot_ref[k : k + 1, :].astype(jnp.float32)).astype(jnp.int32)
            chosen_ref[k, at, :] = jnp.where(ids == wanted, 1.0, 0.0).astype(jnp.bfloat16)
            share_ref[at, k : k + 1] = jax.nn.sigmoid(scores[k] - scores[1 - k])
        return carry

    lax.fori_loop(0, count // piece, choose, 0)
    for u in range(5):
        landed(u)

    tile = slots // 4

    def hide(i, carry):
        at = pl.ds(pl.multiple_of(i * tile, 16), tile)
        gate = jnp.zeros((tile, width), jnp.float32)
        up = jnp.zeros((tile, width), jnp.float32)
        for block in range(NZ):
            v = xall[block, at, :]
            gate = gate + lax.dot_general(v, og[block], ROWS, preferred_element_type=jnp.float32)
            up = up + lax.dot_general(v, ou[block], ROWS, preferred_element_type=jnp.float32)
        inverse = inv_ref[at, :]
        gate = gate * inverse
        up = up * inverse
        hidden[at, :] = (gate / (1.0 + jnp.exp(-gate)) * up).astype(jnp.bfloat16)
        return carry

    lax.fori_loop(0, slots // tile, hide, 0)
    second(5, "ba")
    first(6, "a")

    def block_at(k):
        return lax.rem(z + (2 * lax.rem(k, 2) - 1) * ((k + 1) // 2) + NZ, NZ)

    def half_rows(which):
        return pl.ds(pl.multiple_of(which * half_slots, 16), half_slots)

    def quarter_rows(which, q):
        return pl.ds(pl.multiple_of(which * half_slots + q * quarter, 16), quarter)

    bufs = (theirs, got, mine, joint, far)

    def pair_copy(k, f):
        at = f * NZ + k
        return pltpu.make_async_remote_copy(
            src_ref=bufs[0].at[at],
            dst_ref=bufs[1].at[at],
            send_sem=psend.at[at],
            recv_sem=precv.at[at],
            device_id=partner,
            device_id_type=MESH,
        )

    def home_copy(k, f):
        at = f * NZ + k
        return pltpu.make_async_remote_copy(
            src_ref=bufs[3].at[at],
            dst_ref=parts.at[0, half_rows(core), lanes(f)],
            send_sem=fsend.at[at * 2],
            recv_sem=rrecv.at[f * 9 + 8],
            device_id=partner,
            device_id_type=MESH,
        )

    def far_copy(k, f, q):
        at = f * NZ + k
        return pltpu.make_async_remote_copy(
            src_ref=bufs[3].at[at, pl.ds(q * quarter, quarter), :],
            dst_ref=bufs[4].at[at],
            send_sem=fsend.at[at * 2 + q],
            recv_sem=frecv.at[at * 2 + q],
            device_id=mate(1 - 2 * q),
            device_id_type=MESH,
        )

    def near_copy(k, f, q, side):
        at = f * NZ + k
        return pltpu.make_async_remote_copy(
            src_ref=bufs[3].at[at, pl.ds(q * quarter, quarter), :],
            dst_ref=parts.at[1 + side, quarter_rows(core, q), lanes(f)],
            send_sem=fsend.at[at * 2 + q],
            recv_sem=rrecv.at[f * 9 + side * 4 + core * 2 + q],
            device_id={"tp": block_at(k)},
            device_id_type=MESH,
        )

    def role(k):
        to = block_at(k)
        return to, lax.rem(to // 2 - x + NX, NX)

    def project(k, f):
        at = f * NZ + k
        weights = od[f, block_at(k)]
        bufs[0][at] = lax.dot_general(
            hidden[half_rows(1 - core), :], weights, COLS, preferred_element_type=jnp.float32
        ).astype(jnp.bfloat16)
        pair_copy(k, f).start()
        bufs[2][at] = lax.dot_general(
            hidden[half_rows(core), :], weights, COLS, preferred_element_type=jnp.float32
        ).astype(jnp.bfloat16)

    def project_two(k, f):
        at = f * NZ + k
        weights = jnp.concatenate([od[f, block_at(k)], od[f, block_at(k + 1)]], axis=1)
        for buf, which in ((0, 1 - core), (2, core)):
            value = lax.dot_general(
                hidden[half_rows(which), :], weights, COLS, preferred_element_type=jnp.float32
            ).astype(jnp.bfloat16)
            bufs[buf][at] = value[:, :LANES]
            bufs[buf][at + 1] = value[:, LANES:]
            if buf == 0:
                pair_copy(k, f).start()
                pair_copy(k + 1, f).start()

    def project_both(k):
        block = block_at(k)
        weights = jnp.concatenate([od[0, block], od[1, block]], axis=1)
        for buf, which in ((0, 1 - core), (2, core)):
            value = lax.dot_general(
                hidden[half_rows(which), :], weights, COLS, preferred_element_type=jnp.float32
            ).astype(jnp.bfloat16)
            for f in range(2):
                bufs[buf][f * NZ + k] = value[:, f * LANES : (f + 1) * LANES]
                if buf == 0:
                    pair_copy(k, f).start()

    def join(k, f):
        at = f * NZ + k
        to, which = role(k)
        pair_copy(k, f).wait_recv()
        bufs[3][at] = (
            bufs[2][at].astype(jnp.float32) + bufs[1][at].astype(jnp.float32)
        ).astype(jnp.bfloat16)

        @pl.when(to == tp)
        def _():
            parts[0, half_rows(core), lanes(f)] = bufs[3][at]

        @pl.when((which == 0) & (to != tp))
        def _():
            home_copy(k, f).start()

        @pl.when(which == 2)
        def _():
            far_copy(k, f, 0).start()
            far_copy(k, f, 1).start()

        @pl.when(which == 1)
        def _():
            near_copy(k, f, 1, 0).start()

        @pl.when(which == 3)
        def _():
            near_copy(k, f, 0, 1).start()

    def pass_on(k, f):
        at = f * NZ + k
        _, which = role(k)
        for when, q, side in ((1, 0, 0), (3, 1, 1)):

            @pl.when(which == when)
            def _():
                far_copy(k, f, q).wait_recv()
                piece = pl.ds(q * quarter, quarter)
                bufs[3][at, piece, :] = (
                    bufs[3][at, piece, :].astype(jnp.float32) + bufs[4][at].astype(jnp.float32)
                ).astype(jnp.bfloat16)
                near_copy(k, f, q, side).start()

    def sent(k, f):
        to, which = role(k)
        pair_copy(k, f).wait_send()

        @pl.when((which == 0) & (to != tp))
        def _():
            home_copy(k, f).wait_send()

        @pl.when(which != 0)
        def _():
            far_copy(k, f, 0).wait_send()
            far_copy(k, f, 1).wait_send()

    def near(f):
        project_two(0, f)
        project_two(2, f)
        join(0, f)
        join(1, f)
        project(4, f)
        for k in (2, 3, 4):
            join(k, f)

    def whole_wait(place, sem):
        pltpu.make_async_remote_copy(
            src_ref=place,
            dst_ref=place,
            send_sem=fsend.at[0],
            recv_sem=rrecv.at[sem],
            device_id=partner,
            device_id_type=MESH,
        ).wait_recv()

    def total(c, q, f):
        at = quarter_rows(c, q)
        value = parts[0, at, lanes(f)].astype(jnp.float32)
        for side in range(2):
            whole_wait(parts.at[1 + side, at, lanes(f)], f * 9 + side * 4 + c * 2 + q)
            value = value + parts[1 + side, at, lanes(f)].astype(jnp.float32)
        ret[at, lanes(f)] = value.astype(jnp.bfloat16)

    def give_back(f):
        whole_wait(parts.at[0, half_rows(1 - core), lanes(f)], f * 9 + 8)
        for q, dz in ((0, 1), (1, -1)):
            total(1, q, f)
            for dy in (0, 1, 3, 2):
                back_copy(dz, dy, f).start()
        total(0, 0, f)
        total(0, 1, f)
        for dy in (1, 3, 2):
            back_copy(0, dy, f).start()
        back[here, :, lanes(f)] = ret[arrived_rows(0, y), lanes(f)]

    def each(what, ks, f):
        for k in ks:
            what(k, f)

    close = range(NEAR)
    final = (NEAR, NEAR + 1)
    near(0)
    second(6, "b")
    landed(5, "d")
    project(NZ - 1, 0)
    join(NZ - 1, 0)
    each(pass_on, close, 0)
    landed(5, "c")
    project_two(NEAR, 0)
    each(join, final, 0)
    second(6, "a")
    near(1)
    each(pass_on, (NZ - 1, NEAR, NEAR + 1), 0)
    landed(6, "d")
    project(NZ - 1, 1)
    join(NZ - 1, 1)
    landed(6, "c")
    project_two(NEAR, 1)
    each(join, final, 1)
    each(pass_on, close, 1)
    pass_on(NZ - 1, 1)
    give_back(0)
    each(pass_on, final, 1)
    give_back(1)

    def mix(f):
        def one(i, carry):
            at = pl.ds(pl.multiple_of(i * piece, 16), piece)
            results = back[:, :, lanes(f)].reshape(slots, LANES)
            value = jnp.zeros((piece, LANES), jnp.float32)
            for k in range(2):
                picked = jnp.dot(
                    chosen_ref[k, at, :], results, preferred_element_type=jnp.float32
                )
                value = value + picked * share_ref[at, k : k + 1]
            mix_ref[at, lanes(f)] = value.astype(jnp.bfloat16)
            return carry

        lax.fori_loop(0, count // piece, one, 0)

    for f in range(2):
        for dz, dy in group:
            back_copy(dz, dy, f, True).wait_recv()
        mix(f)

    for u in range(UNITS):
        for dy in (1, 3, 2):
            ycopy(u, dy, y).wait_send()
        for kind in "abcd":
            for sign in (1, -1):
                zcopy(u, kind, sign).wait_send()
    for dz, dy in group:
        tokens_copy(dz, dy).wait_send()
        for f in range(2):
            back_copy(dz, dy, f).wait_send()
    for step in range(1, NX):
        gather_copy(step).wait_send()
    for step in range(NX):
        relay_copy(step).wait_send()
    for f in range(2):
        lax.fori_loop(0, NZ, lambda k, carry: (sent(k, f), carry)[1], 0)


def whole(gate, up, down, gain, tokens, routes, logits):
    _, rows, width = gate.shape
    count, features = tokens.shape
    most = count // 2
    split = [w.reshape(2, NY, rows, width) for w in (gate, up, down)]
    given = (*split, gain, tokens, routes, logits)
    bf16 = jnp.bfloat16
    out = jax.ShapeDtypeStruct((NZ, width, 2 * LANES), bf16)
    dma = lambda n: pltpu.SemaphoreType.DMA((n,))
    vmem = lambda *shape, dtype=bf16: pltpu.VMEM(shape, dtype)
    total = EXPERTS * most
    steps = 2 * NZ
    sums = [vmem(steps, total // 2, LANES)] * 4 + [vmem(steps, total // 4, LANES)]
    return pl.pallas_call(
        whole_kernel,
        out_shape=(
            out,
            out,
            jax.ShapeDtypeStruct((2, NZ, width, LANES), bf16),
            jax.ShapeDtypeStruct((count, features), bf16),
        ),
        in_specs=[pl.BlockSpec(memory_space=pltpu.HBM)] * 7,
        out_specs=(pl.BlockSpec(memory_space=pltpu.VMEM),) * 4,
        scratch_shapes=[
            *[pltpu.VMEM(a.shape, a.dtype) for a in given],
            vmem(2, 2, NY, rows, width),
            vmem(3, 2, NY * rows, width),
            vmem(2, width, 2 * LANES),
            vmem(2, width, LANES),
            vmem(8, count, dtype=jnp.int32),
            vmem(EXPERTS, most, features),
            vmem(2 * NX, total, features),
            vmem(total, 1, dtype=jnp.float32),
            vmem(total, width),
            *sums,
            vmem(3, total, features),
            vmem(total, features),
            vmem(EXPERTS, most, features),
            vmem(2, count, total),
            vmem(count, LANES, dtype=jnp.float32),
            dma(3 * UNITS), dma(3 * UNITS), dma(8 * UNITS), dma(8 * UNITS),
            dma(3 * NY), dma(3 * NY), dma(2 * NX), dma(2 * NX),
            dma(steps), dma(steps), dma(2 * steps), dma(2 * steps), dma(18), dma(6 * NY), dma(6 * NY), dma(7),
        ],
        compiler_params=pltpu.CompilerParams(
            collective_id=0, has_side_effects=True, vmem_limit_bytes=VMEM_LIMIT
        ),
        cost_estimate=pl.CostEstimate(flops=10**11, bytes_accessed=10**7, transcendentals=0),
    )(*[pltpu.with_memory_space_constraint(a, pltpu.HBM) for a in given])


def place_kernel(g_ref, u_ref, d_ref, m_ref, og, ou, od, om, sem):
    copies = [pltpu.make_async_copy(m_ref, om, sem.at[4 * NZ])]
    for m, (ref, out) in enumerate(((g_ref, og), (u_ref, ou))):
        for block in range(NZ):
            columns = pl.ds(block * 2 * LANES, 2 * LANES)
            copies.append(
                pltpu.make_async_copy(ref.at[block], out.at[:, columns], sem.at[m * NZ + block])
            )
    for f in range(2):
        for block in range(NZ):
            columns = pl.ds((block * 2 + f) * LANES, LANES)
            at = (2 + f) * NZ + block
            copies.append(pltpu.make_async_copy(d_ref.at[f, block], od.at[:, columns], sem.at[at]))
    for copy in copies:
        copy.start()
    for copy in copies:
        copy.wait()


def placed_out(blocks):
    nz, width, size = blocks[0].shape
    out = jax.ShapeDtypeStruct((width, nz * size), jnp.bfloat16)
    *turned, mixed = pl.pallas_call(
        place_kernel,
        out_shape=(out, out, out, jax.ShapeDtypeStruct(blocks[3].shape, jnp.bfloat16)),
        in_specs=[pl.BlockSpec(memory_space=pltpu.VMEM)] * 4,
        out_specs=(pl.BlockSpec(memory_space=pl.ANY),) * 4,
        scratch_shapes=[pltpu.SemaphoreType.DMA((4 * NZ + 1,))],
        compiler_params=pltpu.CompilerParams(vmem_limit_bytes=2 * 1024 * 1024),
    )(*blocks)
    return (*[w.T[None] for w in turned], mixed)


def shards(tokens, norm_gain, gate_train, up_train, down_train, routes, route_logits):
    return placed_out(
        whole(
            gate_train, up_train, down_train, norm_gain[None, :], tokens, routes.T, route_logits.T
        )
    )


def solution(mesh):
    placed = (
        P("fs", "tp"),
        P("fs"),
        P(None, "fs", "tp"),
        P(None, "fs", "tp"),
        P(None, "fs", "tp"),
        P("fs", None),
        P("fs", None),
    )
    return jax.shard_map(
        shards,
        mesh=mesh,
        in_specs=placed,
        out_specs=(P("fs", None, "tp"), P("fs", None, "tp"), P("fs", None, "tp"), P("fs", "tp")),
        check_vma=False,
    )
```
